512 devices in a mesh: grp: 2 (over y), ep: 32 (over z, core), tp: 8 (over x).
Axes of the slice: x: 8, y: 2, z: 16, core: 2. Of those that a mesh axis runs over, the one named last changes fastest.
The devices are a block of a 8x8x16 slice.
Arguments:
- value_in: bfloat16 [32768, 1024], P(('grp', 'ep'), 'tp'), parts along dimension 0, may hold values from -6 to 6
- gate_in: bfloat16 [32768, 1024], P(('grp', 'ep'), 'tp'), parts along dimension 0, may hold values from -6 to 6
- conv_taps: float32 [31, 1024], P(None, 'tp'), may hold values from -12 to 12
- chan_gain: float32 [1024], replicated, may hold values from 0.1 to 1.9
- out_weight: bfloat16 [1024, 2048], P(None, 'tp'), may hold values from -0.1875 to 0.1875
- second_rows: bfloat16 [8192, 2048], P(('grp', 'ep')), parts along dimension 0, may hold values from -6 to 6
- expert_gain: float32 [2048], replicated, may hold values from 0.1 to 1.9
- routes: int32 [8192, 2], P(('grp', 'ep')), parts along dimension 0, may hold values from 0 to 15, all different within a row; in each aligned block of 128 rows (0 to 127, 128 to 255, ...) at most 24 rows name the same one
- route_weights: float32 [8192, 2], P(('grp', 'ep')), parts along dimension 0, may hold values from 0.1 to 0.9
- gate_w: bfloat16 [32, 2048, 2048], P('ep', None, 'tp'), may hold values from -0.125 to 0.125
- up_w: bfloat16 [32, 2048, 2048], P('ep', None, 'tp'), may hold values from -0.125 to 0.125
- down_w: bfloat16 [32, 2048, 2048], P('ep', 'tp'), may hold values from -0.125 to 0.125
Outputs:
- mixer_rows: bfloat16 [32768, 2048], P(('grp', 'ep'), 'tp'), parts along dimension 0
- routed_rows: bfloat16 [8192, 2048], P(('grp', 'ep'), 'tp'), parts along dimension 0
The draws below stay inside these ranges and needn't reach their ends.
There are 2 independent parts, one for each index of `grp`. The reference program is written for one: setup_inputs(seed, part) draws one part's arguments, and reference() takes and returns one part's arrays. A program takes and returns all parts, laid end to end along the dimension named above; an argument that names none is the same for every part. Nothing has to cross between parts.
Inputs may be any that keep to these rules, and one draw needn't show every extreme that they name: `routes`: in each aligned block of 128 rows (the rows of one index of ep) no expert is named by more than 24 rows, a bound that some block reaches; each row names 2 different experts.
All inputs are finite; a program needn't handle non-finite values.
Results may differ from the reference program's by a relative error of at most 0.017.
Values may be sent and summed in bfloat16 or wider, within the bound.
No kernel may reach another device: no remote copies, remote signals or barrier semaphores. Data moves between devices by JAX's collectives and lax.ppermute only.
A program may use at most 64 MiB of HBM per device.

```python
import math
import jax
import jax.numpy as jnp
import numpy as np
from jax import lax

D = 2048
CONV_CH = 1024
TAPS = 31
FF_EXPERT = 4096
TOP = 2
TOK_B = 128
HALF_FF = 2048
EXPERTS = 16
CAP = 24
TOKENS_A = 16384
TOKENS_B = 4096
N_EP = 32
N_TP = 8


def draw_conv_taps(key, part):
    channel = jnp.arange(CONV_CH, dtype=jnp.float32)[None, :] / CONV_CH
    rough = jnp.exp(jax.random.uniform(jax.random.fold_in(key, 7), (1, CONV_CH), jnp.float32, -0.5, 0.5))
    base = jnp.clip(jax.random.normal(jax.random.fold_in(key, 5), (TAPS, CONV_CH), jnp.float32), -4.0, 4.0)
    ramp = jnp.exp(jnp.log(3.0) * channel)
    return base * rough * ramp / math.sqrt(TAPS)


def raised(values, stream_key, source, target, shards_of, factor):
    owner, partner = [(jnp.arange(values.shape[position]) // (values.shape[position] // shards_of)).reshape([-1 if axis == position else 1 for axis in range(values.ndim)]) for position in (source, target)]
    chosen = jax.random.permutation(stream_key, shards_of)[partner]
    strong = (owner == chosen) | (owner == (partner + shards_of // 2) % shards_of)
    return jnp.where(strong, factor * values, values)


def level_of(own_key, dims, split, least, high):
    gain, own = 1.0, jax.random.fold_in(own_key, 6)
    for dim, blocks in split:
        heights = jnp.exp(jax.random.uniform(jax.random.fold_in(own, dim), (blocks,), jnp.float32, least / len(split), high / len(split)))
        gain = gain * jnp.repeat(heights, dims[dim] // blocks).reshape([-1 if axis == dim else 1 for axis in range(len(dims))])
    return gain


def shared_out(key, own, number, rows, number_of, top, reach, skew):
    order = jax.random.permutation(key, number_of)
    heavy_load, usual = load_shares(number_of, rows * top, reach, skew, True), load_shares(number_of, rows * top, reach, skew, False)
    places = jnp.arange(number_of)

    def named(sizes, turn):
        used = int((sizes > 0).sum())
        fixed = max(1, used // 4)
        shifted = fixed + (places - fixed + turn * (used - fixed)) % max(1, number_of - fixed)
        return jnp.zeros((number_of,), jnp.int32).at[order[jnp.where(places < fixed, places, shifted)]].set(jnp.asarray(sizes, jnp.int32))

    sizes = jnp.where(number % 4 == 0, named(heavy_load, number // 4), named(usual, number - number // 4 - 1))
    mixed = jax.random.permutation(jax.random.fold_in(own, 3), number_of)
    donor, taker = mixed[0:number_of // 2 * 2:2], mixed[1:number_of // 2 * 2:2]
    slack = jnp.minimum(sizes[donor] - 1, reach - sizes[taker]) // 2
    slack = jnp.where((donor == order[0]) | (taker == order[0]) | (sizes[taker] == 0), 0, jnp.maximum(slack, 0))
    shifted = jax.random.randint(jax.random.fold_in(own, 4), (number_of // 2,), 0, 1 << 20) % (slack + 1)
    sizes = sizes.at[donor].add(-shifted).at[taker].add(shifted)
    members = jnp.searchsorted(jnp.cumsum(sizes), jnp.arange(rows * top), side="right").astype(jnp.int32)
    table = members.reshape(top, rows).T
    table = table[jax.random.permutation(jax.random.fold_in(own, 1), rows)]
    turn = jax.random.randint(jax.random.fold_in(own, 2), (rows, 1), 0, top)
    return jnp.take_along_axis(table, (jnp.arange(top)[None, :] + turn) % top, axis=1)


def load_shares(amount, total, bound, skew, full):
    loads = [(1 << 20) // math.isqrt(rank ** skew) + 1 for rank in range(1, amount + 1)]
    largest = bound if full else min(bound, max(-(-total // amount), total * loads[0] // sum(loads)))
    least = 1 if total - largest >= amount - 1 else 0
    holding, surplus = [largest] + [least] * (amount - 1), total - largest - least * (amount - 1)
    while surplus > 0:
        candidates = [i for i in range(1, amount) if holding[i] < largest] or [i for i in range(1, amount) if holding[i] < bound]
        whole, left = sum([loads[i] for i in candidates]), surplus
        for i in candidates:
            more = min(bound - holding[i], max(1, left * loads[i] // whole), surplus)
            holding[i] = holding[i] + more
            surplus = surplus - more
    return np.array(holding)


def noise(stream_key, extent, deviation, limit, split=(), kind=jnp.bfloat16):
    values = jax.random.normal(stream_key, extent, jnp.float32) * deviation
    if len(split) > 0:
        values = level_of(stream_key, extent, split, -0.22, 0.18) * values
    return jnp.clip(values, min=-limit, max=limit).astype(kind)


def heavy_noise(own_key, shape, spread, most, pieces, heavy, held_as=jnp.bfloat16):
    entries = spread * jax.random.normal(own_key, shape, jnp.float32)
    if pieces:
        entries = entries * level_of(own_key, shape, pieces, -0.22, 0.18)
    return jnp.clip(raised(entries, jax.random.fold_in(own_key, 3), *heavy), -most, most).astype(held_as)


def setup_inputs(seed: int = 0, part: int = 0) -> dict:
    key_list = jax.random.split(jax.random.key(seed), 13)
    part_keys = jax.random.split(jax.random.fold_in(key_list[12], part), 13)
    value_in = noise(part_keys[0], (TOKENS_A, CONV_CH), 1.0, 6.0, ((0, 32), (1, 8)))
    gate_in = noise(part_keys[1], (TOKENS_A, CONV_CH), 1.0, 6.0, ((0, 32), (1, 8)))
    conv_taps = draw_conv_taps(jax.random.fold_in(key_list[12], 71), part)
    chan_gain = jnp.clip(1.0 + 0.18 * jax.random.normal(key_list[3], (CONV_CH,), jnp.float32), 0.1, 1.9)
    out_weight = noise(key_list[4], (CONV_CH, D), CONV_CH ** -0.5, 0.1875, ((1, 8),))
    second_rows = noise(part_keys[5], (TOKENS_B, D), 1.0, 6.0, ((0, 32),))
    expert_gain = jnp.clip(1.0 + 0.18 * jax.random.normal(key_list[6], (D,), jnp.float32), 0.1, 1.9)
    routes_keys = jax.random.split(jax.random.fold_in(part_keys[7], 1), TOKENS_B // TOK_B)
    routes_turns = jax.random.permutation(jax.random.fold_in(part_keys[7], 3), TOKENS_B // TOK_B)
    routes = jax.vmap(lambda own, number: shared_out(jax.random.fold_in(part_keys[7], 2), own, number, TOK_B, EXPERTS, TOP, CAP, 1))(routes_keys, routes_turns).reshape((TOKENS_B, TOP))
    route_weights = jnp.clip(0.1 + 0.79999997 * jax.random.uniform(part_keys[8], (TOKENS_B, TOP), jnp.float32) ** level_of(part_keys[8], (TOKENS_B, TOP), ((0, 32),), -0.2, 0.2), 0.1, 0.9)
    gate_w = noise(key_list[9], (2 * EXPERTS, D, HALF_FF), D ** -0.5, 0.125, ((0, 32), (2, 8)))
    up_w = noise(key_list[10], (2 * EXPERTS, D, HALF_FF), D ** -0.5, 0.125, ((0, 32), (2, 8)))
    down_w = heavy_noise(key_list[11], (2 * EXPERTS, HALF_FF, D), FF_EXPERT ** -0.5, 0.125, ((0, 32), (1, 8)), (1, 2, 8, 2.0))
    return dict(value_in=value_in, gate_in=gate_in, conv_taps=conv_taps, chan_gain=chan_gain, out_weight=out_weight, second_rows=second_rows, expert_gain=expert_gain, routes=routes, route_weights=route_weights, gate_w=gate_w, up_w=up_w, down_w=down_w)


eps = 1e-06

def expert_values(rows, gate_pair, up_pair, down_pair):
    halves = []
    for half in range(2):
        gate = jnp.dot(rows, gate_pair[half], preferred_element_type=jnp.float32)
        upper = jnp.dot(rows, up_pair[half], preferred_element_type=jnp.float32)
        hidden = (jax.nn.silu(gate) * upper).astype(jnp.bfloat16)
        block = hidden.shape[1] // N_TP
        total = jnp.zeros((rows.shape[0], down_pair.shape[2]), jnp.float32)
        for index in range(N_TP):
            piece = jnp.dot(hidden[:, index * block:(index + 1) * block], down_pair[half, index * block:(index + 1) * block], preferred_element_type=jnp.float32)
            total = total + lax.optimization_barrier(piece.astype(jnp.bfloat16)).astype(jnp.float32)
        halves.append(lax.optimization_barrier(total.astype(jnp.bfloat16)).astype(jnp.float32))
    return (halves[0] + halves[1]).astype(jnp.bfloat16)

def reference(value_in, gate_in, conv_taps, chan_gain, out_weight, second_rows, expert_gain, routes, route_weights, gate_w, up_w, down_w):
    glu = (value_in.astype(jnp.float32) * jax.nn.sigmoid(gate_in.astype(jnp.float32))).astype(jnp.bfloat16)
    length = glu.shape[0]
    padded = jnp.concatenate([jnp.zeros((TAPS - 1, glu.shape[1]), jnp.float32), glu.astype(jnp.float32)], axis=0)
    total = jnp.zeros(glu.shape, jnp.float32)
    for offset in range(TAPS):
        total = total + conv_taps[offset][None, :] * padded[offset:offset + length]
    values = total.astype(jnp.bfloat16).astype(jnp.float32)
    centered = values - lax.optimization_barrier(jnp.mean(values, axis=-1, keepdims=True))
    scaled = centered * lax.rsqrt(lax.optimization_barrier(jnp.mean(centered * centered, axis=-1, keepdims=True)) + eps) * chan_gain
    activated = jax.nn.silu(scaled).astype(jnp.bfloat16)
    mixer_rows = jnp.dot(activated, out_weight, preferred_element_type=jnp.float32).astype(jnp.bfloat16)
    rows = second_rows.astype(jnp.float32)
    normed = (rows * lax.rsqrt(lax.optimization_barrier(jnp.mean(rows * rows, axis=-1, keepdims=True)) + eps) * expert_gain).astype(jnp.bfloat16)
    tokens = normed.shape[0]
    chosen = routes.reshape(-1).astype(jnp.int32)
    hits = (chosen[:, None] == jnp.arange(EXPERTS, dtype=jnp.int32)[None, :]).astype(jnp.int32)
    place = lax.optimization_barrier(jnp.sum((jnp.cumsum(hits, axis=0) - 1) * hits, axis=1)).astype(jnp.int32)
    owner = jnp.repeat(jnp.arange(tokens, dtype=jnp.int32), TOP)
    span = N_EP * CAP
    table = jnp.full((EXPERTS, span), tokens, jnp.int32).at[chosen, place].set(owner)
    padded_rows = jnp.concatenate([normed, jnp.zeros((1, normed.shape[1]), jnp.bfloat16)], axis=0)
    gate_pairs = gate_w.reshape(EXPERTS, 2, gate_w.shape[1], gate_w.shape[2])
    up_pairs = up_w.reshape(EXPERTS, 2, up_w.shape[1], up_w.shape[2])
    down_pairs = down_w.reshape(EXPERTS, 2, down_w.shape[1], down_w.shape[2])

    def one_expert(packed):
        index, gate_pair, up_pair, down_pair = packed
        return expert_values(padded_rows[index], gate_pair, up_pair, down_pair)
    outputs = lax.map(one_expert, (table, gate_pairs, up_pairs, down_pairs))
    flat = outputs.reshape(EXPERTS * span, outputs.shape[2])
    picked = flat[(chosen * span + place).astype(jnp.int32)].astype(jnp.float32)
    weighted = picked * route_weights.reshape(-1)[:, None]
    routed_rows = lax.optimization_barrier(jnp.sum(weighted.reshape(tokens, TOP, weighted.shape[1]), axis=1)).astype(jnp.bfloat16)
    return (mixer_rows, routed_rows)
```

```python
import functools

import jax
import jax.numpy as jnp
from jax import lax
from jax.experimental import pallas as pl
from jax.experimental.pallas import tpu as pltpu
from jax.sharding import Mesh
from jax.sharding import PartitionSpec as P

eps = 1e-06
f32 = jnp.float32
bf16 = jnp.bfloat16


def dot(a, b):
    return jnp.dot(a, b, preferred_element_type=f32)


def slot_hits(routes, experts, capacity):
    top, tokens = routes.shape
    expert = lax.broadcasted_iota(jnp.int32, (experts, tokens), 0)
    hits = [(routes[j : j + 1, :] == expert).astype(f32) for j in range(top)]
    named = functools.reduce(jnp.add, hits).astype(bf16)
    before = lax.broadcasted_iota(jnp.int32, (tokens, tokens), 0)
    after = lax.broadcasted_iota(jnp.int32, (tokens, tokens), 1)
    places = dot(named, (before < after).astype(f32).astype(bf16)).astype(bf16)
    slots = experts * capacity
    first = lax.broadcasted_iota(jnp.int32, (slots, experts), 1) * capacity
    slot = lax.broadcasted_iota(jnp.int32, (slots, experts), 0)
    own = (slot >= first) & (slot < first + capacity)
    spread = own.astype(f32).astype(bf16)
    first_of = jnp.sum(jnp.where(own, first, 0), axis=1, keepdims=True)
    offset = (lax.broadcasted_iota(jnp.int32, (slots, 1), 0) - first_of).astype(f32)
    at_place = dot(spread, places) == offset
    return [(dot(spread, hit.astype(bf16)) > 0.5) & at_place for hit in hits]


def dispatch_kernel(experts, capacity, index, routes, rows, gain, out):
    values = rows[...].astype(f32)
    scale = lax.rsqrt(jnp.mean(values * values, axis=-1, keepdims=True) + eps)
    width = out.shape[1]
    start = pl.multiple_of(index[0] * width, width)
    own = rows[:, pl.ds(start, width)].astype(f32)
    normed = (own * scale * gain[:, pl.ds(start, width)]).astype(bf16)
    matches = slot_hits(routes[...], experts, capacity)
    picker = functools.reduce(jnp.logical_or, matches).astype(f32).astype(bf16)
    out[...] = dot(picker, normed).astype(bf16)


def combiner_kernel(experts, capacity, routes, weights, high, low):
    matches = slot_hits(routes[...], experts, capacity)
    terms = [jnp.where(m, weights[j : j + 1, :], 0.0) for j, m in enumerate(matches)]
    total = functools.reduce(jnp.add, terms).T
    rounded = total.astype(bf16)
    high[...] = rounded
    low[...] = (total - rounded.astype(f32)).astype(bf16)


def combine_kernel(high, low, results, out):
    out[...] = (dot(high[...], results[...]) + dot(low[...], results[...])).astype(bf16)


def experts_kernel(x, gate_w, up_w, down_w, out):
    blocks, width = x.shape[1], x.shape[3]
    gate = up = None
    for b in range(blocks):
        part = x[0, b]
        g = dot(part, gate_w[0, b * width : (b + 1) * width, :])
        u = dot(part, up_w[0, b * width : (b + 1) * width, :])
        gate = g if gate is None else gate + g
        up = u if up is None else up + u
    hidden = (jax.nn.silu(gate) * up).astype(bf16)
    for b in range(blocks):
        piece = dot(hidden, down_w[0, :, b * width : (b + 1) * width])
        out[0, b] = piece.astype(bf16)


def mixer_kernel(x, gain, weight, out):
    values = jnp.concatenate([x[b] for b in range(x.shape[0])], axis=1).astype(f32)
    centered = values - jnp.mean(values, axis=-1, keepdims=True)
    scale = lax.rsqrt(jnp.mean(centered * centered, axis=-1, keepdims=True) + eps)
    activated = jax.nn.silu(centered * scale * gain[...]).astype(bf16)
    out[...] = dot(activated, weight[...]).astype(bf16)


def params(mib):
    return pltpu.CompilerParams(vmem_limit_bytes=mib << 20)


def cost(flops, moved):
    return pl.CostEstimate(flops=flops, bytes_accessed=moved, transcendentals=0)


def on_device(
    value_in,
    gate_in,
    conv_taps,
    chan_gain,
    out_weight,
    second_rows,
    expert_gain,
    routes,
    route_weights,
    gate_w,
    up_w,
    down_w,
):
    n_z, n_core, n_tp = lax.axis_size("z"), lax.axis_size("core"), lax.axis_size("tp")
    experts = n_z
    tokens, width = second_rows.shape
    top = routes.shape[1]
    capacity = 2 * max(1, min(tokens // 2, 3 * tokens * top // (4 * experts)))
    columns = width // n_tp
    slots = experts * capacity
    vmem = pl.BlockSpec(memory_space=pltpu.VMEM)
    smem = pl.BlockSpec(memory_space=pltpu.SMEM)

    routes_t = routes.T
    outgoing = pl.pallas_call(
        functools.partial(dispatch_kernel, experts, capacity),
        out_shape=jax.ShapeDtypeStruct((slots, columns), bf16),
        in_specs=[smem, vmem, vmem, vmem],
        out_specs=vmem,
        compiler_params=params(16),
        cost_estimate=cost(10**8, 10**6),
    )(lax.axis_index("tp").reshape(1), routes_t, second_rows, expert_gain.reshape(1, -1))
    arrived = lax.all_to_all(
        outgoing.reshape(experts, capacity, columns), "z", split_axis=0, concat_axis=0, tiled=True
    )
    rows = n_z * capacity
    incoming = lax.all_gather(arrived.reshape(1, rows, columns), ("core", "tp"), axis=0, tiled=True)

    taps = conv_taps.shape[0]
    halo = -(-(taps - 1) // 16) * 16
    glu = (value_in.astype(f32) * jax.nn.sigmoid(gate_in.astype(f32))).astype(bf16)
    length, channels = glu.shape
    n_ep = n_z * n_core
    before = lax.ppermute(
        glu[length - halo :], ("z", "core"), [(i, i + 1) for i in range(n_ep - 1)]
    )
    padded = jnp.concatenate([before, glu], axis=0).astype(f32)
    total = jnp.zeros(glu.shape, f32)
    for offset in range(taps):
        start = halo - taps + 1 + offset
        total = total + conv_taps[offset][None, :] * padded[start : start + length]
    convolved = total.astype(bf16)
    gathered = lax.all_gather(convolved, "tp", axis=0, tiled=False)
    step = length // 2
    mixer_rows = pl.pallas_call(
        mixer_kernel,
        grid=(length // step,),
        out_shape=jax.ShapeDtypeStruct((length, out_weight.shape[1]), bf16),
        in_specs=[
            pl.BlockSpec((n_tp, step, channels), lambda i: (0, i, 0)),
            pl.BlockSpec((1, n_tp * channels), lambda i: (0, 0)),
            pl.BlockSpec(out_weight.shape, lambda i: (0, 0)),
        ],
        out_specs=pl.BlockSpec((step, out_weight.shape[1]), lambda i: (i, 0)),
        compiler_params=params(16),
        cost_estimate=cost(10**9, 2 * 10**6),
    )(gathered, chan_gain.reshape(1, -1), out_weight)

    step = rows // 2
    block = (1, n_tp, step, columns)
    whole = lambda i: (0, 0, 0)
    pieces = pl.pallas_call(
        experts_kernel,
        grid=(n_core * 2,),
        out_shape=jax.ShapeDtypeStruct((n_core, n_tp, rows, columns), bf16),
        in_specs=[
            pl.BlockSpec(block, lambda i: (i // 2, 0, i % 2, 0)),
            pl.BlockSpec(gate_w.shape, whole),
            pl.BlockSpec(up_w.shape, whole),
            pl.BlockSpec(down_w.shape, whole),
        ],
        out_specs=pl.BlockSpec(block, lambda i: (i // 2, 0, i % 2, 0)),
        compiler_params=params(24),
        cost_estimate=cost(3 * 10**9, 10**7),
    )(incoming.reshape(n_core, n_tp, rows, columns), gate_w, up_w, down_w)
    sums = lax.psum_scatter(
        pieces.reshape(n_core * n_tp, rows, columns), ("core", "tp"), scatter_dimension=0, tiled=True
    )
    results = lax.all_to_all(
        sums.reshape(n_z, capacity, columns), "z", split_axis=0, concat_axis=0, tiled=True
    ).reshape(slots, columns)

    high, low = pl.pallas_call(
        functools.partial(combiner_kernel, experts, capacity),
        out_shape=[jax.ShapeDtypeStruct((tokens, slots), bf16)] * 2,
        in_specs=[vmem] * 2,
        out_specs=[vmem] * 2,
        compiler_params=params(16),
        cost_estimate=cost(10**8, 10**6),
    )(routes_t, route_weights.T)
    routed_rows = pl.pallas_call(
        combine_kernel,
        out_shape=jax.ShapeDtypeStruct((tokens, columns), bf16),
        in_specs=[vmem] * 3,
        out_specs=vmem,
        compiler_params=params(16),
        cost_estimate=cost(10**8, 10**6),
    )(high, low, results)
    return (mixer_rows, routed_rows)


def solution(mesh):
    n_grp, n_ep, n_tp = (mesh.shape[name] for name in ("grp", "ep", "tp"))
    finer = Mesh(mesh.devices.reshape(n_grp, n_ep // 2, 2, n_tp), ("grp", "z", "core", "tp"))
    tok = ("grp", "z", "core")
    placed = (
        P(tok, "tp"),
        P(tok, "tp"),
        P(None, "tp"),
        P(),
        P(None, "tp"),
        P(tok, None),
        P(),
        P(tok, None),
        P(tok, None),
        P(("z", "core"), None, "tp"),
        P(("z", "core"), None, "tp"),
        P(("z", "core"), "tp", None),
    )
    return jax.shard_map(
        on_device,
        mesh=finer,
        in_specs=placed,
        out_specs=(P(tok, "tp"), P(tok, "tp")),
        check_vma=False,
    )
```

```python
import functools

import jax
import jax.numpy as jnp
from jax import lax
from jax.experimental import pallas as pl
from jax.experimental.pallas import tpu as pltpu
from jax.sharding import Mesh
from jax.sharding import PartitionSpec as P

eps = 1e-06
f32 = jnp.float32
bf16 = jnp.bfloat16


def dot(a, b):
    return jnp.dot(a, b, preferred_element_type=f32)


def slot_hits(routes, experts, capacity):
    top, tokens = routes.shape
    expert = lax.broadcasted_iota(jnp.int32, (experts, tokens), 0)
    hits = [(routes[j : j + 1, :] == expert).astype(f32) for j in range(top)]
    named = functools.reduce(jnp.add, hits).astype(bf16)
    before = lax.broadcasted_iota(jnp.int32, (tokens, tokens), 0)
    after = lax.broadcasted_iota(jnp.int32, (tokens, tokens), 1)
    places = dot(named, (before < after).astype(f32).astype(bf16)).astype(bf16)
    slots = experts * capacity
    first = lax.broadcasted_iota(jnp.int32, (slots, experts), 1) * capacity
    slot = lax.broadcasted_iota(jnp.int32, (slots, experts), 0)
    own = (slot >= first) & (slot < first + capacity)
    spread = own.astype(f32).astype(bf16)
    first_of = jnp.sum(jnp.where(own, first, 0), axis=1, keepdims=True)
    offset = (lax.broadcasted_iota(jnp.int32, (slots, 1), 0) - first_of).astype(f32)
    at_place = dot(spread, places) == offset
    return [(dot(spread, hit.astype(bf16)) > 0.5) & at_place for hit in hits]


def dispatch_kernel(experts, capacity, index, routes, rows, gain, out):
    values = rows[...].astype(f32)
    scale = lax.rsqrt(jnp.mean(values * values, axis=-1, keepdims=True) + eps)
    width = out.shape[1]
    start = pl.multiple_of(index[0] * width, width)
    own = rows[:, pl.ds(start, width)].astype(f32)
    normed = (own * scale * gain[:, pl.ds(start, width)]).astype(bf16)
    matches = slot_hits(routes[...], experts, capacity)
    picker = functools.reduce(jnp.logical_or, matches).astype(f32).astype(bf16)
    out[...] = dot(picker, normed).astype(bf16)


def combiner_kernel(experts, capacity, routes, weights, high, low):
    matches = slot_hits(routes[...], experts, capacity)
    terms = [jnp.where(m, weights[j : j + 1, :], 0.0) for j, m in enumerate(matches)]
    total = functools.reduce(jnp.add, terms).T
    rounded = total.astype(bf16)
    high[...] = rounded
    low[...] = (total - rounded.astype(f32)).astype(bf16)


def combine_kernel(high, low, results, out):
    out[...] = (dot(high[...], results[...]) + dot(low[...], results[...])).astype(bf16)


def experts_kernel(x, gate_0, up_0, gate_1, up_1, down_0, down_1, out, wide, tall, sems):
    blocks, width = x.shape[0], x.shape[2]
    span = lambda b: slice(b * width, (b + 1) * width)
    held = [wide.at[i] for i in range(4)] + [tall.at[i] for i in range(2)]
    weights = (gate_0, up_0, gate_1, up_1, down_0, down_1)
    copies = [
        pltpu.make_async_copy(w.at[0], h, sems.at[i]) for i, (w, h) in enumerate(zip(weights, held))
    ]
    for copy in copies:
        copy.start()

    def projected(i):
        copies[i].wait()
        return functools.reduce(jnp.add, [dot(x[b], held[i][span(b), :]) for b in range(blocks)])

    hidden = []
    for half in range(2):
        gate = projected(2 * half)
        hidden.append((jax.nn.silu(gate) * projected(2 * half + 1)).astype(bf16))
    copies[4].wait()
    copies[5].wait()
    for b in range(blocks):
        piece = dot(hidden[0], held[4][:, span(b)]) + dot(hidden[1], held[5][:, span(b)])
        out[b] = piece.astype(bf16)


def sum_kernel(pieces, out):
    total = pieces[0].astype(f32)
    for b in range(1, pieces.shape[0]):
        total = total + pieces[b].astype(f32)
    out[...] = total.astype(bf16)


def mixer_kernel(x, gain, weight, out):
    values = jnp.concatenate([x[b] for b in range(x.shape[0])], axis=1).astype(f32)
    centered = values - jnp.mean(values, axis=-1, keepdims=True)
    scale = lax.rsqrt(jnp.mean(centered * centered, axis=-1, keepdims=True) + eps)
    activated = jax.nn.silu(centered * scale * gain[...]).astype(bf16)
    out[...] = dot(activated, weight[...]).astype(bf16)


def from_each(value, axis):
    copies = jnp.broadcast_to(value, (lax.axis_size(axis), *value.shape))
    return lax.all_to_all(copies, axis, split_axis=0, concat_axis=0, tiled=True)


def partner(value):
    return lax.ppermute(value, "core", [(0, 1), (1, 0)])


def params(mib):
    return pltpu.CompilerParams(vmem_limit_bytes=mib << 20)


def cost(flops, moved):
    return pl.CostEstimate(flops=flops, bytes_accessed=moved, transcendentals=0)


def on_device(
    value_in,
    gate_in,
    conv_taps,
    chan_gain,
    out_weight,
    second_rows,
    expert_gain,
    routes,
    route_weights,
    gate_w,
    up_w,
    down_w,
):
    n_z, n_core, n_tp = lax.axis_size("z"), lax.axis_size("core"), lax.axis_size("tp")
    experts = n_z
    tokens, width = second_rows.shape
    top = routes.shape[1]
    capacity = 2 * max(1, min(tokens // 2, 3 * tokens * top // (4 * experts)))
    columns = width // n_tp
    slots = experts * capacity
    vmem = pl.BlockSpec(memory_space=pltpu.VMEM)
    smem = pl.BlockSpec(memory_space=pltpu.SMEM)

    routes_t = routes.T
    outgoing = pl.pallas_call(
        functools.partial(dispatch_kernel, experts, capacity),
        out_shape=jax.ShapeDtypeStruct((slots, columns), bf16),
        in_specs=[smem, vmem, vmem, vmem],
        out_specs=vmem,
        compiler_params=params(16),
        cost_estimate=cost(10**8, 10**6),
    )(lax.axis_index("tp").reshape(1), routes_t, second_rows, expert_gain.reshape(1, -1))
    arrived = lax.all_to_all(
        outgoing.reshape(experts, capacity, columns), "z", split_axis=0, concat_axis=0, tiled=True
    )
    rows = n_z * capacity
    gate_b, up_b, down_b = (partner(w) for w in (gate_w, up_w, down_w))

    taps = conv_taps.shape[0]
    halo = -(-(taps - 1) // 16) * 16
    glu = (value_in.astype(f32) * jax.nn.sigmoid(gate_in.astype(f32))).astype(bf16)
    length, channels = glu.shape
    n_ep = n_z * n_core
    before = lax.ppermute(
        glu[length - halo :], ("z", "core"), [(i, i + 1) for i in range(n_ep - 1)]
    )
    padded = jnp.concatenate([before, glu], axis=0).astype(f32)
    total = jnp.zeros(glu.shape, f32)
    for offset in range(taps):
        start = halo - taps + 1 + offset
        total = total + conv_taps[offset][None, :] * padded[start : start + length]
    convolved = total.astype(bf16)
    gathered = from_each(convolved, "tp")
    arrived, gathered, gate_b, up_b, down_b = lax.optimization_barrier(
        (arrived, gathered, gate_b, up_b, down_b)
    )
    incoming = from_each(arrived.reshape(rows, columns), "tp")
    step = length // 2
    mixer_rows = pl.pallas_call(
        mixer_kernel,
        grid=(length // step,),
        out_shape=jax.ShapeDtypeStruct((length, out_weight.shape[1]), bf16),
        in_specs=[
            pl.BlockSpec((n_tp, step, channels), lambda i: (0, i, 0)),
            pl.BlockSpec((1, n_tp * channels), lambda i: (0, 0)),
            pl.BlockSpec(out_weight.shape, lambda i: (0, 0)),
        ],
        out_specs=pl.BlockSpec((step, out_weight.shape[1]), lambda i: (i, 0)),
        compiler_params=params(16),
        cost_estimate=cost(10**9, 2 * 10**6),
    )(gathered, chan_gain.reshape(1, -1), out_weight)

    hbm = pl.BlockSpec(memory_space=pl.ANY)
    units = gate_w.shape[2]
    pieces = pl.pallas_call(
        experts_kernel,
        out_shape=jax.ShapeDtypeStruct((n_tp, rows, columns), bf16),
        in_specs=[vmem] + [hbm] * 6,
        out_specs=vmem,
        scratch_shapes=[
            pltpu.VMEM((4, width, units), bf16),
            pltpu.VMEM((2, units, width), bf16),
            pltpu.SemaphoreType.DMA((6,)),
        ],
        compiler_params=params(56),
        cost_estimate=cost(3 * 10**9, 10**7),
    )(incoming, gate_w, up_w, gate_b, up_b, down_w, down_b)
    pieces = lax.all_to_all(pieces, "tp", split_axis=0, concat_axis=0, tiled=True)
    step = rows // 2
    sums = pl.pallas_call(
        sum_kernel,
        grid=(rows // step,),
        out_shape=jax.ShapeDtypeStruct((rows, columns), bf16),
        in_specs=[pl.BlockSpec((n_tp, step, columns), lambda i: (0, i, 0))],
        out_specs=pl.BlockSpec((step, columns), lambda i: (i, 0)),
        compiler_params=params(16),
        cost_estimate=cost(10**8, 2 * 10**6),
    )(pieces)
    results = lax.all_to_all(
        sums.reshape(n_z, capacity, columns), "z", split_axis=0, concat_axis=0, tiled=True
    ).reshape(slots, columns)

    high, low = pl.pallas_call(
        functools.partial(combiner_kernel, experts, capacity),
        out_shape=[jax.ShapeDtypeStruct((tokens, slots), bf16)] * 2,
        in_specs=[vmem] * 2,
        out_specs=[vmem] * 2,
        compiler_params=params(16),
        cost_estimate=cost(10**8, 10**6),
    )(routes_t, route_weights.T)
    routed_rows = pl.pallas_call(
        combine_kernel,
        out_shape=jax.ShapeDtypeStruct((tokens, columns), bf16),
        in_specs=[vmem] * 3,
        out_specs=vmem,
        compiler_params=params(16),
        cost_estimate=cost(10**8, 10**6),
    )(high, low, results)
    return (mixer_rows, routed_rows)


def solution(mesh):
    n_grp, n_ep, n_tp = (mesh.shape[name] for name in ("grp", "ep", "tp"))
    finer = Mesh(mesh.devices.reshape(n_grp, n_ep // 2, 2, n_tp), ("grp", "z", "core", "tp"))
    tok = ("grp", "z", "core")
    placed = (
        P(tok, "tp"),
        P(tok, "tp"),
        P(None, "tp"),
        P(),
        P(None, "tp"),
        P(tok, None),
        P(),
        P(tok, None),
        P(tok, None),
        P(("z", "core"), None, "tp"),
        P(("z", "core"), None, "tp"),
        P(("z", "core"), "tp", None),
    )
    return jax.shard_map(
        on_device,
        mesh=finer,
        in_specs=placed,
        out_specs=(P(tok, "tp"), P(tok, "tp")),
        check_vma=False,
    )
```

```python
import functools

import jax
import jax.numpy as jnp
from jax import lax
from jax.experimental import pallas as pl
from jax.experimental.pallas import tpu as pltpu
from jax.sharding import Mesh
from jax.sharding import PartitionSpec as P


eps = 1e-06
f32 = jnp.float32
bf16 = jnp.bfloat16


def dot(a, b):
    return jnp.dot(a, b, preferred_element_type=f32)


def slot_hits(routes, experts, capacity):
    top, tokens = routes.shape
    expert = lax.broadcasted_iota(jnp.int32, (experts, tokens), 0)
    hits = [(routes[j : j + 1, :] == expert).astype(f32) for j in range(top)]
    named = functools.reduce(jnp.add, hits).astype(bf16)
    before = lax.broadcasted_iota(jnp.int32, (tokens, tokens), 0)
    after = lax.broadcasted_iota(jnp.int32, (tokens, tokens), 1)
    places = dot(named, (before < after).astype(f32).astype(bf16)).astype(bf16)
    slots = experts * capacity
    first = lax.broadcasted_iota(jnp.int32, (slots, experts), 1) * capacity
    slot = lax.broadcasted_iota(jnp.int32, (slots, experts), 0)
    own = (slot >= first) & (slot < first + capacity)
    spread = own.astype(f32).astype(bf16)
    first_of = jnp.sum(jnp.where(own, first, 0), axis=1, keepdims=True)
    offset = (lax.broadcasted_iota(jnp.int32, (slots, 1), 0) - first_of).astype(f32)
    at_place = dot(spread, places) == offset
    return [(dot(spread, hit.astype(bf16)) > 0.5) & at_place for hit in hits]


def dispatch_kernel(experts, capacity, index, routes, rows, gain, out):
    values = rows[...].astype(f32)
    scale = lax.rsqrt(jnp.mean(values * values, axis=-1, keepdims=True) + eps)
    width = out.shape[1]
    start = pl.multiple_of(index[0] * width, width)
    own = rows[:, pl.ds(start, width)].astype(f32)
    normed = (own * scale * gain[:, pl.ds(start, width)]).astype(bf16)
    matches = slot_hits(routes[...], experts, capacity)
    picker = functools.reduce(jnp.logical_or, matches).astype(f32).astype(bf16)
    out[...] = dot(picker, normed).astype(bf16)


def combiner_kernel(experts, capacity, routes, weights, high, low):
    matches = slot_hits(routes[...], experts, capacity)
    terms = [jnp.where(m, weights[j : j + 1, :], 0.0) for j, m in enumerate(matches)]
    total = functools.reduce(jnp.add, terms).T
    rounded = total.astype(bf16)
    high[...] = rounded
    low[...] = (total - rounded.astype(f32)).astype(bf16)


def combine_kernel(high, low, results, out):
    out[...] = (dot(high[...], results[...]) + dot(low[...], results[...])).astype(bf16)


def experts_kernel(
    index, x_0, x_1, x_3, x_2a, x_2b, gate_0, up_0, gate_1, up_1, down_0, down_1, out, wide, tall, sems
):
    blocks, width = out.shape[0], out.shape[2]
    held = [wide.at[i] for i in range(4)] + [tall.at[i] for i in range(2)]
    weights = (gate_0, up_0, gate_1, up_1, down_0, down_1)
    copies = [
        pltpu.make_async_copy(w.at[0], h, sems.at[i]) for i, (w, h) in enumerate(zip(weights, held))
    ]
    for copy in copies:
        copy.start()
    depth = x_0.shape[1]
    parts = wide.shape[1] // depth
    rows = (x_0[...], x_1[...], jnp.concatenate([x_2a[...], x_2b[...]], axis=0), x_3[...])
    places = [lax.rem(index[0] + k, parts) * depth for k in range(parts)]

    def projected(i):
        copies[i].wait()
        terms = [
            dot(r, held[i][pl.ds(pl.multiple_of(p, depth), depth), :]) for r, p in zip(rows, places)
        ]
        return functools.reduce(jnp.add, terms)

    hidden = []
    for half in range(2):
        gate = projected(2 * half)
        hidden.append((jax.nn.silu(gate) * projected(2 * half + 1)).astype(bf16))
    copies[4].wait()
    copies[5].wait()
    for b in range(blocks):
        span = slice(b * width, (b + 1) * width)
        piece = dot(hidden[0], held[4][:, span]) + dot(hidden[1], held[5][:, span])
        out[b] = piece.astype(bf16)


def sum_kernel(pieces, out):
    total = pieces[0].astype(f32)
    for b in range(1, pieces.shape[0]):
        total = total + pieces[b].astype(f32)
    out[...] = total.astype(bf16)


def mixer_kernel(index, *refs):
    *pieces, gain, weight, out = refs
    n, width = len(pieces), pieces[0].shape[1]
    values = jnp.concatenate([p[...] for p in pieces], axis=1).astype(f32)
    spans = [
        pl.ds(pl.multiple_of(lax.rem(index[0] + n - k, n) * width, width), width) for k in range(n)
    ]
    gains = jnp.concatenate([gain[:, span] for span in spans], axis=1)
    weights = jnp.concatenate([weight[span, :] for span in spans], axis=0)
    centered = values - jnp.mean(values, axis=-1, keepdims=True)
    scale = lax.rsqrt(jnp.mean(centered * centered, axis=-1, keepdims=True) + eps)
    activated = jax.nn.silu(centered * scale * gains).astype(bf16)
    out[...] = dot(activated, weights).astype(bf16)


def moved(value, by):
    n = lax.axis_size("tp")
    return lax.ppermute(value, "tp", [(i, (i + by) % n) for i in range(n)])


def partner(value):
    return lax.ppermute(value, "core", [(0, 1), (1, 0)])


def params(mib):
    return pltpu.CompilerParams(vmem_limit_bytes=mib << 20)


def cost(flops, moved):
    return pl.CostEstimate(flops=flops, bytes_accessed=moved, transcendentals=0)


def step_on_device(
    value_in,
    gate_in,
    conv_taps,
    chan_gain,
    out_weight,
    second_rows,
    expert_gain,
    routes,
    route_weights,
    gate_w,
    up_w,
    down_w,
):
    n_z, n_core, n_tp = lax.axis_size("z"), lax.axis_size("core"), lax.axis_size("tp")
    experts = n_z
    tokens, width = second_rows.shape
    top = routes.shape[1]
    capacity = 2 * max(1, min(tokens // 2, 3 * tokens * top // (4 * experts)))
    columns = width // n_tp
    slots = experts * capacity
    vmem = pl.BlockSpec(memory_space=pltpu.VMEM)
    smem = pl.BlockSpec(memory_space=pltpu.SMEM)

    routes_t = routes.T
    me = lax.axis_index("tp")
    parts = n_tp // 2
    wide = width // parts
    quarter = lax.rem(me, parts).astype(jnp.int32).reshape(1)
    outgoing = pl.pallas_call(
        functools.partial(dispatch_kernel, experts, capacity),
        grid=(1,),
        out_shape=jax.ShapeDtypeStruct((slots, wide), bf16),
        in_specs=[smem] + [pl.BlockSpec(s, lambda i: (0, 0)) for s in ((top, tokens), (tokens, width), (1, width))],
        out_specs=pl.BlockSpec((slots, wide), lambda i: (0, 0)),
        compiler_params=params(60),
        cost_estimate=cost(10**8, 10**6),
    )(quarter, routes_t, second_rows, expert_gain.reshape(1, -1))
    arrived = lax.all_to_all(
        outgoing.reshape(experts, capacity, wide), "z", split_axis=0, concat_axis=0, tiled=True
    )

    value_in, gate_in, outgoing = lax.optimization_barrier((value_in, gate_in, outgoing))
    taps = conv_taps.shape[0]
    halo = -(-(taps - 1) // 16) * 16
    glu = (value_in.astype(f32) * jax.nn.sigmoid(gate_in.astype(f32))).astype(bf16)
    length, channels = glu.shape
    n_ep = n_z * n_core
    before = lax.ppermute(
        glu[length - halo :], ("z", "core"), [(i, i + 1) for i in range(n_ep - 1)]
    )
    padded = jnp.concatenate([before, glu], axis=0).astype(f32)
    total = jnp.zeros(glu.shape, f32)
    for offset in range(taps):
        start = halo - taps + 1 + offset
        total = total + conv_taps[offset][None, :] * padded[start : start + length]
    convolved = total.astype(bf16)
    from_back = [moved(convolved, k) for k in range(1, parts)]
    from_front = [moved(convolved, -k) for k in range(1, parts)]

    rows = n_z * capacity
    arrived, from_back, from_front = lax.optimization_barrier((arrived, from_back, from_front))
    x_0 = arrived.reshape(rows, wide)
    x_2a, x_2b = moved(x_0[: rows // 2], -2), moved(x_0[rows // 2 :], 2)
    x_1, x_3 = moved(x_0, -1), moved(x_0, 1)
    own = lax.optimization_barrier((x_0, gate_w, up_w, down_w))
    gate_b, up_b, down_b = (partner(w) for w in own[1:])
    hbm = pl.BlockSpec(memory_space=pl.ANY)
    units = gate_w.shape[2]
    pieces = pl.pallas_call(
        experts_kernel,
        out_shape=jax.ShapeDtypeStruct((n_tp, rows, columns), bf16),
        in_specs=[smem] + [vmem] * 5 + [hbm] * 6,
        out_specs=vmem,
        scratch_shapes=[
            pltpu.VMEM((4, width, units), bf16),
            pltpu.VMEM((2, units, width), bf16),
            pltpu.SemaphoreType.DMA((6,)),
        ],
        compiler_params=params(24),
        cost_estimate=cost(3 * 10**9, 10**7),
    )(quarter, x_0, x_1, x_3, x_2a, x_2b, gate_w, up_w, gate_b, up_b, down_w, down_b)
    pieces = lax.all_to_all(pieces, "tp", split_axis=0, concat_axis=0, tiled=True)
    step = rows // 2
    sums = pl.pallas_call(
        sum_kernel,
        grid=(rows // step,),
        out_shape=jax.ShapeDtypeStruct((rows, columns), bf16),
        in_specs=[pl.BlockSpec((n_tp, step, columns), lambda i: (0, i, 0))],
        out_specs=pl.BlockSpec((step, columns), lambda i: (i, 0)),
        compiler_params=params(16),
        cost_estimate=cost(10**8, 2 * 10**6),
    )(pieces)
    sums, convolved = lax.optimization_barrier((sums, convolved))
    across = moved(convolved, parts)
    results = lax.all_to_all(
        sums.reshape(n_z, capacity, columns), "z", split_axis=0, concat_axis=0, tiled=True
    ).reshape(slots, columns)

    high, low = pl.pallas_call(
        functools.partial(combiner_kernel, experts, capacity),
        out_shape=[jax.ShapeDtypeStruct((tokens, slots), bf16)] * 2,
        in_specs=[vmem] * 2,
        out_specs=[vmem] * 2,
        compiler_params=params(16),
        cost_estimate=cost(10**8, 10**6),
    )(routes_t, route_weights.T)
    routed_rows = pl.pallas_call(
        combine_kernel,
        out_shape=jax.ShapeDtypeStruct((tokens, columns), bf16),
        in_specs=[vmem] * 3,
        out_specs=vmem,
        compiler_params=params(16),
        cost_estimate=cost(10**8, 10**6),
    )(high, low, results)
    step = length // 2
    gathered = [convolved, *from_back, across, *from_front[::-1]]
    mixer_rows = pl.pallas_call(
        mixer_kernel,
        grid=(length // step,),
        out_shape=jax.ShapeDtypeStruct((length, out_weight.shape[1]), bf16),
        in_specs=[smem]
        + [pl.BlockSpec((step, channels), lambda i: (i, 0))] * n_tp
        + [
            pl.BlockSpec((1, n_tp * channels), lambda i: (0, 0)),
            pl.BlockSpec(out_weight.shape, lambda i: (0, 0)),
        ],
        out_specs=pl.BlockSpec((step, out_weight.shape[1]), lambda i: (i, 0)),
        compiler_params=params(16),
        cost_estimate=cost(10**9, 2 * 10**6),
    )(me.astype(jnp.int32).reshape(1), *gathered, chan_gain.reshape(1, -1), out_weight)
    return (mixer_rows, routed_rows)


def solution(mesh):
    n_grp, n_ep, n_tp = (mesh.shape[name] for name in ("grp", "ep", "tp"))
    finer = Mesh(mesh.devices.reshape(n_grp, n_ep // 2, 2, n_tp), ("grp", "z", "core", "tp"))
    tok = ("grp", "z", "core")
    placed = (
        P(tok, "tp"),
        P(tok, "tp"),
        P(None, "tp"),
        P(),
        P(None, "tp"),
        P(tok, None),
        P(),
        P(tok, None),
        P(tok, None),
        P(("z", "core"), None, "tp"),
        P(("z", "core"), None, "tp"),
        P(("z", "core"), "tp", None),
    )
    return jax.shard_map(
        step_on_device,
        mesh=finer,
        in_specs=placed,
        out_specs=(P(tok, "tp"), P(tok, "tp")),
        check_vma=False,
    )
```

```python
import functools

import jax
import jax.numpy as jnp
from jax import lax
from jax.experimental import pallas as pl
from jax.experimental.pallas import tpu as pltpu
from jax.sharding import Mesh
from jax.sharding import PartitionSpec as P


eps = 1e-06
f32 = jnp.float32
bf16 = jnp.bfloat16


def dot(a, b):
    return jnp.dot(a, b, preferred_element_type=f32)


def slot_hits(routes, experts, capacity):
    top, tokens = routes.shape
    expert = lax.broadcasted_iota(jnp.int32, (experts, tokens), 0)
    hits = [(routes[j : j + 1, :] == expert).astype(f32) for j in range(top)]
    named = functools.reduce(jnp.add, hits).astype(bf16)
    before = lax.broadcasted_iota(jnp.int32, (tokens, tokens), 0)
    after = lax.broadcasted_iota(jnp.int32, (tokens, tokens), 1)
    places = dot(named, (before < after).astype(f32).astype(bf16)).astype(bf16)
    slots = experts * capacity
    first = lax.broadcasted_iota(jnp.int32, (slots, experts), 1) * capacity
    slot = lax.broadcasted_iota(jnp.int32, (slots, experts), 0)
    own = (slot >= first) & (slot < first + capacity)
    spread = own.astype(f32).astype(bf16)
    first_of = jnp.sum(jnp.where(own, first, 0), axis=1, keepdims=True)
    offset = (lax.broadcasted_iota(jnp.int32, (slots, 1), 0) - first_of).astype(f32)
    at_place = dot(spread, places) == offset
    return [(dot(spread, hit.astype(bf16)) > 0.5) & at_place for hit in hits]


def dispatch_kernel(experts, capacity, index, routes, rows, gain, out):
    values = rows[...].astype(f32)
    scale = lax.rsqrt(jnp.mean(values * values, axis=-1, keepdims=True) + eps)
    width = out.shape[1]
    start = pl.multiple_of(index[0] * width, width)
    own = rows[:, pl.ds(start, width)].astype(f32)
    normed = (own * scale * gain[:, pl.ds(start, width)]).astype(bf16)
    matches = slot_hits(routes[...], experts, capacity)
    picker = functools.reduce(jnp.logical_or, matches).astype(f32).astype(bf16)
    out[...] = dot(picker, normed).astype(bf16)


def combiner_kernel(experts, capacity, routes, weights, high, low):
    matches = slot_hits(routes[...], experts, capacity)
    terms = [jnp.where(m, weights[j : j + 1, :], 0.0) for j, m in enumerate(matches)]
    total = functools.reduce(jnp.add, terms).T
    rounded = total.astype(bf16)
    high[...] = rounded
    low[...] = (total - rounded.astype(f32)).astype(bf16)


def combine_kernel(high, low, results, out):
    out[...] = (dot(high[...], results[...]) + dot(low[...], results[...])).astype(bf16)


def experts_kernel(
    index, x_0, x_1, x_3, x_2a, x_2b, gate_0, up_0, gate_1, up_1, down_0, down_1, out, wide, tall, held_out, sems, out_sems
):
    blocks, width = out.shape[0], out.shape[2]
    held = [wide.at[i] for i in range(4)] + [tall.at[i] for i in range(2)]
    weights = (gate_0, up_0, gate_1, up_1, down_0, down_1)
    copies = [
        pltpu.make_async_copy(w.at[0], h, sems.at[i]) for i, (w, h) in enumerate(zip(weights, held))
    ]
    for copy in copies:
        copy.start()
    depth = x_0.shape[1]
    parts = wide.shape[1] // depth
    rows = (x_0[...], x_1[...], jnp.concatenate([x_2a[...], x_2b[...]], axis=0), x_3[...])
    places = [lax.rem(index[0] + k, parts) * depth for k in range(parts)]

    def projected(i):
        copies[i].wait()
        terms = [
            dot(r, held[i][pl.ds(pl.multiple_of(p, depth), depth), :]) for r, p in zip(rows, places)
        ]
        return functools.reduce(jnp.add, terms)

    hidden = []
    for half in range(2):
        gate = projected(2 * half)
        hidden.append((jax.nn.silu(gate) * projected(2 * half + 1)).astype(bf16))
    copies[4].wait()
    copies[5].wait()
    stores = []
    for b in range(blocks):
        span = slice(b * width, (b + 1) * width)
        piece = dot(hidden[0], held[4][:, span]) + dot(hidden[1], held[5][:, span])
        held_out[b] = piece.astype(bf16)
        stores.append(pltpu.make_async_copy(held_out.at[b], out.at[b], out_sems.at[b]))
        stores[-1].start()
    for store in stores:
        store.wait()


def mixer_kernel(x, gain, weight, out):
    values = jnp.concatenate([x[b] for b in range(x.shape[0])], axis=1).astype(f32)
    centered = values - jnp.mean(values, axis=-1, keepdims=True)
    scale = lax.rsqrt(jnp.mean(centered * centered, axis=-1, keepdims=True) + eps)
    activated = jax.nn.silu(centered * scale * gain[...]).astype(bf16)
    out[...] = dot(activated, weight[...]).astype(bf16)


def moved(value, by):
    n = lax.axis_size("tp")
    return lax.ppermute(value, "tp", [(i, (i + by) % n) for i in range(n)])


def partner(value):
    return lax.ppermute(value, "core", [(0, 1), (1, 0)])


def params(mib):
    return pltpu.CompilerParams(vmem_limit_bytes=mib << 20)


def cost(flops, moved):
    return pl.CostEstimate(flops=flops, bytes_accessed=moved, transcendentals=0)


def step_on_device(
    value_in,
    gate_in,
    conv_taps,
    chan_gain,
    out_weight,
    second_rows,
    expert_gain,
    routes,
    route_weights,
    gate_w,
    up_w,
    down_w,
):
    n_z, n_core, n_tp = lax.axis_size("z"), lax.axis_size("core"), lax.axis_size("tp")
    experts = n_z
    tokens, width = second_rows.shape
    top = routes.shape[1]
    capacity = 2 * max(1, min(tokens // 2, 3 * tokens * top // (4 * experts)))
    columns = width // n_tp
    slots = experts * capacity
    vmem = pl.BlockSpec(memory_space=pltpu.VMEM)
    smem = pl.BlockSpec(memory_space=pltpu.SMEM)

    routes_t = routes.T
    me = lax.axis_index("tp")
    parts = n_tp // 2
    wide = width // parts
    quarter = lax.rem(me, parts).astype(jnp.int32).reshape(1)
    outgoing = pl.pallas_call(
        functools.partial(dispatch_kernel, experts, capacity),
        grid=(1,),
        out_shape=jax.ShapeDtypeStruct((slots, wide), bf16),
        in_specs=[smem] + [pl.BlockSpec(s, lambda i: (0, 0)) for s in ((top, tokens), (tokens, width), (1, width))],
        out_specs=pl.BlockSpec((slots, wide), lambda i: (0, 0)),
        compiler_params=params(60),
        cost_estimate=cost(10**8, 10**6),
    )(quarter, routes_t, second_rows, expert_gain.reshape(1, -1))
    arrived = lax.all_to_all(
        outgoing.reshape(experts, capacity, wide), "z", split_axis=0, concat_axis=0, tiled=True
    )

    own = (value_in, gate_in, gate_w, up_w, down_w)
    value_in, gate_in, *own, outgoing = lax.optimization_barrier((*own, outgoing))
    taps = conv_taps.shape[0]
    halo = -(-(taps - 1) // 16) * 16
    glu = (value_in.astype(f32) * jax.nn.sigmoid(gate_in.astype(f32))).astype(bf16)
    length, channels = glu.shape
    n_ep = n_z * n_core
    before = lax.ppermute(
        glu[length - halo :], ("z", "core"), [(i, i + 1) for i in range(n_ep - 1)]
    )
    gate_b, up_b, down_b = (partner(w) for w in own)
    padded = jnp.concatenate([before, glu], axis=0).astype(f32)
    total = jnp.zeros(glu.shape, f32)
    for offset in range(taps):
        start = halo - taps + 1 + offset
        total = total + conv_taps[offset][None, :] * padded[start : start + length]
    convolved = total.astype(bf16)
    arrived, _ = lax.optimization_barrier((arrived, convolved))
    gathered = lax.all_gather(convolved, "tp", axis=0, tiled=False)

    rows = n_z * capacity
    x_0 = arrived.reshape(rows, wide)
    x_2a, x_2b = moved(x_0[: rows // 2], -2), moved(x_0[rows // 2 :], 2)
    x_1, x_3 = moved(x_0, -1), moved(x_0, 1)
    hbm = pl.BlockSpec(memory_space=pl.ANY)
    units = gate_w.shape[2]
    pieces = pl.pallas_call(
        experts_kernel,
        out_shape=jax.ShapeDtypeStruct((n_tp, rows, columns), bf16),
        in_specs=[smem] + [vmem] * 5 + [hbm] * 6,
        out_specs=hbm,
        scratch_shapes=[
            pltpu.VMEM((4, width, units), bf16),
            pltpu.VMEM((2, units, width), bf16),
            pltpu.VMEM((n_tp, rows, columns), bf16),
            pltpu.SemaphoreType.DMA((6,)),
            pltpu.SemaphoreType.DMA((n_tp,)),
        ],
        compiler_params=params(24),
        cost_estimate=cost(3 * 10**9, 10**7),
    )(quarter, x_0, x_1, x_3, x_2a, x_2b, gate_w, up_w, gate_b, up_b, down_w, down_b)
    sums = lax.psum_scatter(pieces, "tp", scatter_dimension=0, tiled=True)
    results = lax.all_to_all(
        sums.reshape(n_z, capacity, columns), "z", split_axis=0, concat_axis=0, tiled=True
    ).reshape(slots, columns)

    high, low = pl.pallas_call(
        functools.partial(combiner_kernel, experts, capacity),
        out_shape=[jax.ShapeDtypeStruct((tokens, slots), bf16)] * 2,
        in_specs=[vmem] * 2,
        out_specs=[vmem] * 2,
        compiler_params=params(16),
        cost_estimate=cost(10**8, 10**6),
    )(routes_t, route_weights.T)
    routed_rows = pl.pallas_call(
        combine_kernel,
        out_shape=jax.ShapeDtypeStruct((tokens, columns), bf16),
        in_specs=[vmem] * 3,
        out_specs=vmem,
        compiler_params=params(16),
        cost_estimate=cost(10**8, 10**6),
    )(high, low, results)
    step = length // 2
    mixer_rows = pl.pallas_call(
        mixer_kernel,
        grid=(length // step,),
        out_shape=jax.ShapeDtypeStruct((length, out_weight.shape[1]), bf16),
        in_specs=[
            pl.BlockSpec((n_tp, step, channels), lambda i: (0, i, 0)),
            pl.BlockSpec((1, n_tp * channels), lambda i: (0, 0)),
            pl.BlockSpec(out_weight.shape, lambda i: (0, 0)),
        ],
        out_specs=pl.BlockSpec((step, out_weight.shape[1]), lambda i: (i, 0)),
        compiler_params=params(16),
        cost_estimate=cost(10**9, 2 * 10**6),
    )(gathered, chan_gain.reshape(1, -1), out_weight)

    return (mixer_rows, routed_rows)


def solution(mesh):
    n_grp, n_ep, n_tp = (mesh.shape[name] for name in ("grp", "ep", "tp"))
    finer = Mesh(mesh.devices.reshape(n_grp, n_ep // 2, 2, n_tp), ("grp", "z", "core", "tp"))
    tok = ("grp", "z", "core")
    placed = (
        P(tok, "tp"),
        P(tok, "tp"),
        P(None, "tp"),
        P(),
        P(None, "tp"),
        P(tok, None),
        P(),
        P(tok, None),
        P(tok, None),
        P(("z", "core"), None, "tp"),
        P(("z", "core"), None, "tp"),
        P(("z", "core"), "tp", None),
    )
    return jax.shard_map(
        step_on_device,
        mesh=finer,
        in_specs=placed,
        out_specs=(P(tok, "tp"), P(tok, "tp")),
        check_vma=False,
    )
```

```python
import functools

import jax
import jax.numpy as jnp
from jax import lax
from jax.experimental import pallas as pl
from jax.experimental.pallas import tpu as pltpu
from jax.sharding import Mesh
from jax.sharding import PartitionSpec as P


eps = 1e-06
f32 = jnp.float32
bf16 = jnp.bfloat16


def dot(a, b):
    return jnp.dot(a, b, preferred_element_type=f32)


def slot_hits(routes, experts, capacity):
    top, tokens = routes.shape
    expert = lax.broadcasted_iota(jnp.int32, (experts, tokens), 0)
    hits = [(routes[j : j + 1, :] == expert).astype(f32) for j in range(top)]
    named = functools.reduce(jnp.add, hits).astype(bf16)
    before = lax.broadcasted_iota(jnp.int32, (tokens, tokens), 0)
    after = lax.broadcasted_iota(jnp.int32, (tokens, tokens), 1)
    places = dot(named, (before < after).astype(f32).astype(bf16)).astype(bf16)
    slots = experts * capacity
    first = lax.broadcasted_iota(jnp.int32, (slots, experts), 1) * capacity
    slot = lax.broadcasted_iota(jnp.int32, (slots, experts), 0)
    own = (slot >= first) & (slot < first + capacity)
    spread = own.astype(f32).astype(bf16)
    first_of = jnp.sum(jnp.where(own, first, 0), axis=1, keepdims=True)
    offset = (lax.broadcasted_iota(jnp.int32, (slots, 1), 0) - first_of).astype(f32)
    at_place = dot(spread, places) == offset
    return [(dot(spread, hit.astype(bf16)) > 0.5) & at_place for hit in hits]


def dispatch_kernel(experts, capacity, index, routes, rows, gain, out):
    values = rows[...].astype(f32)
    scale = lax.rsqrt(jnp.mean(values * values, axis=-1, keepdims=True) + eps)
    width = out.shape[1]
    start = pl.multiple_of(index[0] * width, width)
    own = rows[:, pl.ds(start, width)].astype(f32)
    normed = (own * scale * gain[:, pl.ds(start, width)]).astype(bf16)
    matches = slot_hits(routes[...], experts, capacity)
    picker = functools.reduce(jnp.logical_or, matches).astype(f32).astype(bf16)
    out[...] = dot(picker, normed).astype(bf16)


def combiner_kernel(experts, capacity, routes, weights, high, low):
    matches = slot_hits(routes[...], experts, capacity)
    terms = [jnp.where(m, weights[j : j + 1, :], 0.0) for j, m in enumerate(matches)]
    total = functools.reduce(jnp.add, terms).T
    rounded = total.astype(bf16)
    high[...] = rounded
    low[...] = (total - rounded.astype(f32)).astype(bf16)


def combine_kernel(high, low, results, out):
    out[...] = (dot(high[...], results[...]) + dot(low[...], results[...])).astype(bf16)


def experts_kernel(
    index, x_0, x_1, x_3, x_2a, x_2b, gate_0, up_0, gate_1, up_1, down_0, down_1, out, wide, tall, held_out, sems, out_sems
):
    blocks, width = out.shape[0], out.shape[2]
    held = [wide.at[i] for i in range(4)] + [tall.at[i] for i in range(2)]
    weights = (gate_0, up_0, gate_1, up_1, down_0, down_1)
    copies = [
        pltpu.make_async_copy(w.at[0], h, sems.at[i]) for i, (w, h) in enumerate(zip(weights, held))
    ]
    for copy in copies:
        copy.start()
    depth = x_0.shape[1]
    parts = wide.shape[1] // depth
    rows = (x_0[...], x_1[...], jnp.concatenate([x_2a[...], x_2b[...]], axis=0), x_3[...])
    places = [lax.rem(index[0] + k, parts) * depth for k in range(parts)]

    def projected(i):
        copies[i].wait()
        terms = [
            dot(r, held[i][pl.ds(pl.multiple_of(p, depth), depth), :]) for r, p in zip(rows, places)
        ]
        return functools.reduce(jnp.add, terms)

    hidden = []
    for half in range(2):
        gate = projected(2 * half)
        hidden.append((jax.nn.silu(gate) * projected(2 * half + 1)).astype(bf16))
    copies[4].wait()
    copies[5].wait()
    stores = []
    for b in range(blocks):
        span = slice(b * width, (b + 1) * width)
        piece = dot(hidden[0], held[4][:, span]) + dot(hidden[1], held[5][:, span])
        held_out[b] = piece.astype(bf16)
        stores.append(pltpu.make_async_copy(held_out.at[b], out.at[b], out_sems.at[b]))
        stores[-1].start()
    for store in stores:
        store.wait()


def sum_kernel(pieces, out):
    total = pieces[0].astype(f32)
    for b in range(1, pieces.shape[0]):
        total = total + pieces[b].astype(f32)
    out[...] = total.astype(bf16)


def mixer_kernel(index, *refs):
    *pieces, gain, weight, out = refs
    n, width = len(pieces), pieces[0].shape[1]
    values = jnp.concatenate([p[...] for p in pieces], axis=1).astype(f32)
    spans = [
        pl.ds(pl.multiple_of(lax.rem(index[0] + n - k, n) * width, width), width) for k in range(n)
    ]
    gains = jnp.concatenate([gain[:, span] for span in spans], axis=1)
    weights = jnp.concatenate([weight[span, :] for span in spans], axis=0)
    centered = values - jnp.mean(values, axis=-1, keepdims=True)
    scale = lax.rsqrt(jnp.mean(centered * centered, axis=-1, keepdims=True) + eps)
    activated = jax.nn.silu(centered * scale * gains).astype(bf16)
    out[...] = dot(activated, weights).astype(bf16)


def moved(value, by):
    n = lax.axis_size("tp")
    return lax.ppermute(value, "tp", [(i, (i + by) % n) for i in range(n)])


def partner(value):
    return lax.ppermute(value, "core", [(0, 1), (1, 0)])


def params(mib):
    return pltpu.CompilerParams(vmem_limit_bytes=mib << 20)


def cost(flops, moved):
    return pl.CostEstimate(flops=flops, bytes_accessed=moved, transcendentals=0)


def step_on_device(
    value_in,
    gate_in,
    conv_taps,
    chan_gain,
    out_weight,
    second_rows,
    expert_gain,
    routes,
    route_weights,
    gate_w,
    up_w,
    down_w,
):
    n_z, n_core, n_tp = lax.axis_size("z"), lax.axis_size("core"), lax.axis_size("tp")
    experts = n_z
    tokens, width = second_rows.shape
    top = routes.shape[1]
    capacity = 2 * max(1, min(tokens // 2, 3 * tokens * top // (4 * experts)))
    columns = width // n_tp
    slots = experts * capacity
    vmem = pl.BlockSpec(memory_space=pltpu.VMEM)
    smem = pl.BlockSpec(memory_space=pltpu.SMEM)

    routes_t = routes.T
    me = lax.axis_index("tp")
    parts = n_tp // 2
    wide = width // parts
    quarter = lax.rem(me, parts).astype(jnp.int32).reshape(1)
    outgoing = pl.pallas_call(
        functools.partial(dispatch_kernel, experts, capacity),
        grid=(1,),
        out_shape=jax.ShapeDtypeStruct((slots, wide), bf16),
        in_specs=[smem] + [pl.BlockSpec(s, lambda i: (0, 0)) for s in ((top, tokens), (tokens, width), (1, width))],
        out_specs=pl.BlockSpec((slots, wide), lambda i: (0, 0)),
        compiler_params=params(60),
        cost_estimate=cost(10**8, 10**6),
    )(quarter, routes_t, second_rows, expert_gain.reshape(1, -1))
    arrived = lax.all_to_all(
        outgoing.reshape(experts, capacity, wide), "z", split_axis=0, concat_axis=0, tiled=True
    )

    taps = conv_taps.shape[0]
    halo = -(-(taps - 1) // 16) * 16
    glu = (value_in.astype(f32) * jax.nn.sigmoid(gate_in.astype(f32))).astype(bf16)
    length, channels = glu.shape
    n_ep = n_z * n_core
    before = lax.ppermute(
        glu[length - halo :], ("z", "core"), [(i, i + 1) for i in range(n_ep - 1)]
    )
    padded = jnp.concatenate([before, glu], axis=0).astype(f32)
    total = jnp.zeros(glu.shape, f32)
    for offset in range(taps):
        start = halo - taps + 1 + offset
        total = total + conv_taps[offset][None, :] * padded[start : start + length]
    convolved = total.astype(bf16)
    across = moved(convolved, parts)
    from_back = [moved(convolved, k) for k in range(1, parts - 1)]
    from_front = [moved(convolved, -k) for k in range(1, parts - 1)]
    from_back.append(moved(convolved, parts - 1))
    from_front.append(moved(convolved, 1 - parts))

    rows = n_z * capacity
    arrived, _ = lax.optimization_barrier((arrived, convolved))
    x_0 = arrived.reshape(rows, wide)
    x_2a, x_2b = moved(x_0[: rows // 2], -2), moved(x_0[rows // 2 :], 2)
    x_1, x_3 = moved(x_0, -1), moved(x_0, 1)
    gate_b, up_b, down_b = (partner(w) for w in (gate_w, up_w, down_w))
    hbm = pl.BlockSpec(memory_space=pl.ANY)
    units = gate_w.shape[2]
    pieces = pl.pallas_call(
        experts_kernel,
        out_shape=jax.ShapeDtypeStruct((n_tp, rows, columns), bf16),
        in_specs=[smem] + [vmem] * 5 + [hbm] * 6,
        out_specs=hbm,
        scratch_shapes=[
            pltpu.VMEM((4, width, units), bf16),
            pltpu.VMEM((2, units, width), bf16),
            pltpu.VMEM((n_tp, rows, columns), bf16),
            pltpu.SemaphoreType.DMA((6,)),
            pltpu.SemaphoreType.DMA((n_tp,)),
        ],
        compiler_params=params(24),
        cost_estimate=cost(3 * 10**9, 10**7),
    )(quarter, x_0, x_1, x_3, x_2a, x_2b, gate_w, up_w, gate_b, up_b, down_w, down_b)
    pieces = lax.all_to_all(pieces, "tp", split_axis=0, concat_axis=0, tiled=True)
    step = rows // 2
    sums = pl.pallas_call(
        sum_kernel,
        grid=(rows // step,),
        out_shape=jax.ShapeDtypeStruct((rows, columns), bf16),
        in_specs=[pl.BlockSpec((n_tp, step, columns), lambda i: (0, i, 0))],
        out_specs=pl.BlockSpec((step, columns), lambda i: (i, 0)),
        compiler_params=params(16),
        cost_estimate=cost(10**8, 2 * 10**6),
    )(pieces)
    results = lax.all_to_all(
        sums.reshape(n_z, capacity, columns), "z", split_axis=0, concat_axis=0, tiled=True
    ).reshape(slots, columns)

    high, low = pl.pallas_call(
        functools.partial(combiner_kernel, experts, capacity),
        out_shape=[jax.ShapeDtypeStruct((tokens, slots), bf16)] * 2,
        in_specs=[vmem] * 2,
        out_specs=[vmem] * 2,
        compiler_params=params(16),
        cost_estimate=cost(10**8, 10**6),
    )(routes_t, route_weights.T)
    routed_rows = pl.pallas_call(
        combine_kernel,
        out_shape=jax.ShapeDtypeStruct((tokens, columns), bf16),
        in_specs=[vmem] * 3,
        out_specs=vmem,
        compiler_params=params(16),
        cost_estimate=cost(10**8, 10**6),
    )(high, low, results)
    step = length // 2
    gathered = [convolved, *from_back, across, *from_front[::-1]]
    mixer_rows = pl.pallas_call(
        mixer_kernel,
        grid=(length // step,),
        out_shape=jax.ShapeDtypeStruct((length, out_weight.shape[1]), bf16),
        in_specs=[smem]
        + [pl.BlockSpec((step, channels), lambda i: (i, 0))] * n_tp
        + [
            pl.BlockSpec((1, n_tp * channels), lambda i: (0, 0)),
            pl.BlockSpec(out_weight.shape, lambda i: (0, 0)),
        ],
        out_specs=pl.BlockSpec((step, out_weight.shape[1]), lambda i: (i, 0)),
        compiler_params=params(16),
        cost_estimate=cost(10**9, 2 * 10**6),
    )(me.astype(jnp.int32).reshape(1), *gathered, chan_gain.reshape(1, -1), out_weight)
    return (mixer_rows, routed_rows)


def solution(mesh):
    n_grp, n_ep, n_tp = (mesh.shape[name] for name in ("grp", "ep", "tp"))
    finer = Mesh(mesh.devices.reshape(n_grp, n_ep // 2, 2, n_tp), ("grp", "z", "core", "tp"))
    tok = ("grp", "z", "core")
    placed = (
        P(tok, "tp"),
        P(tok, "tp"),
        P(None, "tp"),
        P(),
        P(None, "tp"),
        P(tok, None),
        P(),
        P(tok, None),
        P(tok, None),
        P(("z", "core"), None, "tp"),
        P(("z", "core"), None, "tp"),
        P(("z", "core"), "tp", None),
    )
    return jax.shard_map(
        step_on_device,
        mesh=finer,
        in_specs=placed,
        out_specs=(P(tok, "tp"), P(tok, "tp")),
        check_vma=False,
    )
```

```python
import functools

import jax
import jax.numpy as jnp
from jax import lax
from jax.experimental import pallas as pl
from jax.experimental.pallas import tpu as pltpu
from jax.sharding import Mesh
from jax.sharding import PartitionSpec as P


eps = 1e-06
f32 = jnp.float32
bf16 = jnp.bfloat16


def dot(a, b):
    return jnp.dot(a, b, preferred_element_type=f32)


def slot_hits(routes, experts, capacity):
    top, tokens = routes.shape
    expert = lax.broadcasted_iota(jnp.int32, (experts, tokens), 0)
    hits = [(routes[j : j + 1, :] == expert).astype(f32) for j in range(top)]
    named = functools.reduce(jnp.add, hits).astype(bf16)
    before = lax.broadcasted_iota(jnp.int32, (tokens, tokens), 0)
    after = lax.broadcasted_iota(jnp.int32, (tokens, tokens), 1)
    places = dot(named, (before < after).astype(f32).astype(bf16)).astype(bf16)
    slots = experts * capacity
    first = lax.broadcasted_iota(jnp.int32, (slots, experts), 1) * capacity
    slot = lax.broadcasted_iota(jnp.int32, (slots, experts), 0)
    own = (slot >= first) & (slot < first + capacity)
    spread = own.astype(f32).astype(bf16)
    first_of = jnp.sum(jnp.where(own, first, 0), axis=1, keepdims=True)
    offset = (lax.broadcasted_iota(jnp.int32, (slots, 1), 0) - first_of).astype(f32)
    at_place = dot(spread, places) == offset
    return [(dot(spread, hit.astype(bf16)) > 0.5) & at_place for hit in hits]


def dispatch_kernel(experts, capacity, index, routes, rows, gain, out):
    values = rows[...].astype(f32)
    scale = lax.rsqrt(jnp.mean(values * values, axis=-1, keepdims=True) + eps)
    width = out.shape[1]
    start = pl.multiple_of(index[0] * width, width)
    own = rows[:, pl.ds(start, width)].astype(f32)
    normed = (own * scale * gain[:, pl.ds(start, width)]).astype(bf16)
    matches = slot_hits(routes[...], experts, capacity)
    picker = functools.reduce(jnp.logical_or, matches).astype(f32).astype(bf16)
    out[...] = dot(picker, normed).astype(bf16)


def combiner_kernel(experts, capacity, routes, weights, high, low):
    matches = slot_hits(routes[...], experts, capacity)
    terms = [jnp.where(m, weights[j : j + 1, :], 0.0) for j, m in enumerate(matches)]
    total = functools.reduce(jnp.add, terms).T
    rounded = total.astype(bf16)
    high[...] = rounded
    low[...] = (total - rounded.astype(f32)).astype(bf16)


def combine_kernel(high, low, results, out):
    out[...] = (dot(high[...], results[...]) + dot(low[...], results[...])).astype(bf16)


def experts_kernel(
    index, x_0, x_1, x_3, x_2a, x_2b, gate_0, up_0, down_0, gate_1, up_1, down_1, out, wide, tall, held_out, sems, out_sems
):
    blocks, width = out.shape[0], out.shape[2]
    arriving = (wide.at[0], wide.at[1], tall)
    copies = [
        pltpu.make_async_copy(w.at[0], h, sems.at[i])
        for i, (w, h) in enumerate(zip((gate_1, up_1, down_1), arriving))
    ]
    for copy in copies:
        copy.start()
    depth = x_0.shape[1]
    parts = gate_0.shape[1] // depth
    rows = (x_0[...], x_1[...], jnp.concatenate([x_2a[...], x_2b[...]], axis=0), x_3[...])
    places = [lax.rem(index[0] + k, parts) * depth for k in range(parts)]

    def projected(weight):
        spans = [pl.ds(pl.multiple_of(p, depth), depth) for p in places]
        return functools.reduce(jnp.add, [dot(r, weight[s, :]) for r, s in zip(rows, spans)])

    gate = projected(gate_0.at[0])
    hidden = [(jax.nn.silu(gate) * projected(up_0.at[0])).astype(bf16)]
    copies[0].wait()
    gate = projected(wide.at[0])
    copies[1].wait()
    hidden.append((jax.nn.silu(gate) * projected(wide.at[1])).astype(bf16))
    copies[2].wait()
    stores = []
    for b in range(blocks):
        span = slice(b * width, (b + 1) * width)
        piece = dot(hidden[0], down_0[0, :, span]) + dot(hidden[1], tall[:, span])
        held_out[b] = piece.astype(bf16)
        stores.append(pltpu.make_async_copy(held_out.at[b], out.at[b], out_sems.at[b]))
        stores[-1].start()
    for store in stores:
        store.wait()


def sum_kernel(pieces, out):
    total = pieces[0].astype(f32)
    for b in range(1, pieces.shape[0]):
        total = total + pieces[b].astype(f32)
    out[...] = total.astype(bf16)


def mixer_kernel(index, *refs):
    *pieces, gain, weight, out = refs
    n, width = len(pieces), pieces[0].shape[1]
    values = jnp.concatenate([p[...] for p in pieces], axis=1).astype(f32)
    spans = [
        pl.ds(pl.multiple_of(lax.rem(index[0] + n - k, n) * width, width), width) for k in range(n)
    ]
    gains = jnp.concatenate([gain[:, span] for span in spans], axis=1)
    weights = jnp.concatenate([weight[span, :] for span in spans], axis=0)
    centered = values - jnp.mean(values, axis=-1, keepdims=True)
    scale = lax.rsqrt(jnp.mean(centered * centered, axis=-1, keepdims=True) + eps)
    activated = jax.nn.silu(centered * scale * gains).astype(bf16)
    out[...] = dot(activated, weights).astype(bf16)


def moved(value, by):
    n = lax.axis_size("tp")
    return lax.ppermute(value, "tp", [(i, (i + by) % n) for i in range(n)])


def partner(value):
    return lax.ppermute(value, "core", [(0, 1), (1, 0)])


def params(mib):
    return pltpu.CompilerParams(vmem_limit_bytes=mib << 20)


def cost(flops, moved):
    return pl.CostEstimate(flops=flops, bytes_accessed=moved, transcendentals=0)


def step_on_device(
    value_in,
    gate_in,
    conv_taps,
    chan_gain,
    out_weight,
    second_rows,
    expert_gain,
    routes,
    route_weights,
    gate_w,
    up_w,
    down_w,
):
    n_z, n_core, n_tp = lax.axis_size("z"), lax.axis_size("core"), lax.axis_size("tp")
    experts = n_z
    tokens, width = second_rows.shape
    top = routes.shape[1]
    capacity = 2 * max(1, min(tokens // 2, 3 * tokens * top // (4 * experts)))
    columns = width // n_tp
    slots = experts * capacity
    vmem = pl.BlockSpec(memory_space=pltpu.VMEM)
    smem = pl.BlockSpec(memory_space=pltpu.SMEM)

    routes_t = routes.T
    me = lax.axis_index("tp")
    parts = n_tp // 2
    wide = width // parts
    quarter = lax.rem(me, parts).astype(jnp.int32).reshape(1)
    outgoing = pl.pallas_call(
        functools.partial(dispatch_kernel, experts, capacity),
        grid=(1,),
        out_shape=jax.ShapeDtypeStruct((slots, wide), bf16),
        in_specs=[smem] + [pl.BlockSpec(s, lambda i: (0, 0)) for s in ((top, tokens), (tokens, width), (1, width))],
        out_specs=pl.BlockSpec((slots, wide), lambda i: (0, 0)),
        compiler_params=params(60),
        cost_estimate=cost(10**8, 10**6),
    )(quarter, routes_t, second_rows, expert_gain.reshape(1, -1))
    arrived = lax.all_to_all(
        outgoing.reshape(experts, capacity, wide), "z", split_axis=0, concat_axis=0, tiled=True
    )

    taps = conv_taps.shape[0]
    halo = -(-(taps - 1) // 16) * 16
    glu = (value_in.astype(f32) * jax.nn.sigmoid(gate_in.astype(f32))).astype(bf16)
    length, channels = glu.shape
    n_ep = n_z * n_core
    before = lax.ppermute(
        glu[length - halo :], ("z", "core"), [(i, i + 1) for i in range(n_ep - 1)]
    )
    padded = jnp.concatenate([before, glu], axis=0).astype(f32)
    total = jnp.zeros(glu.shape, f32)
    for offset in range(taps):
        start = halo - taps + 1 + offset
        total = total + conv_taps[offset][None, :] * padded[start : start + length]
    convolved = total.astype(bf16)
    across, from_back = moved(convolved, parts), [moved(convolved, k) for k in (1, 2)]
    from_front = [moved(convolved, -k) for k in range(1, parts)]
    from_back.append(moved(convolved, parts - 1))

    rows = n_z * capacity
    arrived, _ = lax.optimization_barrier((arrived, convolved))
    x_0 = arrived.reshape(rows, wide)
    x_2a, x_2b = moved(x_0[: rows // 2], -2), moved(x_0[rows // 2 :], 2)
    x_1, x_3 = moved(x_0, -1), moved(x_0, 1)
    gate_b, up_b, down_b = (partner(w) for w in (gate_w, up_w, down_w))
    hbm = pl.BlockSpec(memory_space=pl.ANY)
    units = gate_w.shape[2]
    pieces = pl.pallas_call(
        experts_kernel,
        out_shape=jax.ShapeDtypeStruct((n_tp, rows, columns), bf16),
        in_specs=[smem] + [vmem] * 8 + [hbm] * 3,
        out_specs=hbm,
        scratch_shapes=[
            pltpu.VMEM((2, width, units), bf16),
            pltpu.VMEM((units, width), bf16),
            pltpu.VMEM((n_tp, rows, columns), bf16),
            pltpu.SemaphoreType.DMA((3,)),
            pltpu.SemaphoreType.DMA((n_tp,)),
        ],
        compiler_params=params(24),
        cost_estimate=cost(3 * 10**9, 10**7),
    )(quarter, x_0, x_1, x_3, x_2a, x_2b, gate_w, up_w, down_w, gate_b, up_b, down_b)
    pieces = lax.all_to_all(pieces, "tp", split_axis=0, concat_axis=0, tiled=True)
    pieces, from_front = lax.optimization_barrier((pieces, from_front))
    step = rows // 2
    sums = pl.pallas_call(
        sum_kernel,
        grid=(rows // step,),
        out_shape=jax.ShapeDtypeStruct((rows, columns), bf16),
        in_specs=[pl.BlockSpec((n_tp, step, columns), lambda i: (0, i, 0))],
        out_specs=pl.BlockSpec((step, columns), lambda i: (i, 0)),
        compiler_params=params(16),
        cost_estimate=cost(10**8, 2 * 10**6),
    )(pieces)
    results = lax.all_to_all(
        sums.reshape(n_z, capacity, columns), "z", split_axis=0, concat_axis=0, tiled=True
    ).reshape(slots, columns)

    high, low = pl.pallas_call(
        functools.partial(combiner_kernel, experts, capacity),
        out_shape=[jax.ShapeDtypeStruct((tokens, slots), bf16)] * 2,
        in_specs=[vmem] * 2,
        out_specs=[vmem] * 2,
        compiler_params=params(16),
        cost_estimate=cost(10**8, 10**6),
    )(routes_t, route_weights.T)
    routed_rows = pl.pallas_call(
        combine_kernel,
        out_shape=jax.ShapeDtypeStruct((tokens, columns), bf16),
        in_specs=[vmem] * 3,
        out_specs=vmem,
        compiler_params=params(16),
        cost_estimate=cost(10**8, 10**6),
    )(high, low, results)
    step = length // 2
    gathered = [convolved, *from_back, across, *from_front[::-1]]
    mixer_rows = pl.pallas_call(
        mixer_kernel,
        grid=(length // step,),
        out_shape=jax.ShapeDtypeStruct((length, out_weight.shape[1]), bf16),
        in_specs=[smem]
        + [pl.BlockSpec((step, channels), lambda i: (i, 0))] * n_tp
        + [
            pl.BlockSpec((1, n_tp * channels), lambda i: (0, 0)),
            pl.BlockSpec(out_weight.shape, lambda i: (0, 0)),
        ],
        out_specs=pl.BlockSpec((step, out_weight.shape[1]), lambda i: (i, 0)),
        compiler_params=params(16),
        cost_estimate=cost(10**9, 2 * 10**6),
    )(me.astype(jnp.int32).reshape(1), *gathered, chan_gain.reshape(1, -1), out_weight)
    return (mixer_rows, routed_rows)


def solution(mesh):
    n_grp, n_ep, n_tp = (mesh.shape[name] for name in ("grp", "ep", "tp"))
    finer = Mesh(mesh.devices.reshape(n_grp, n_ep // 2, 2, n_tp), ("grp", "z", "core", "tp"))
    tok = ("grp", "z", "core")
    placed = (
        P(tok, "tp"),
        P(tok, "tp"),
        P(None, "tp"),
        P(),
        P(None, "tp"),
        P(tok, None),
        P(),
        P(tok, None),
        P(tok, None),
        P(("z", "core"), None, "tp"),
        P(("z", "core"), None, "tp"),
        P(("z", "core"), "tp", None),
    )
    return jax.shard_map(
        step_on_device,
        mesh=finer,
        in_specs=placed,
        out_specs=(P(tok, "tp"), P(tok, "tp")),
        check_vma=False,
    )
```

```python
import functools

import jax
import jax.numpy as jnp
from jax import lax
from jax.experimental import pallas as pl
from jax.experimental.pallas import tpu as pltpu
from jax.sharding import Mesh
from jax.sharding import PartitionSpec as P


eps = 1e-06
f32 = jnp.float32
bf16 = jnp.bfloat16


def dot(a, b):
    return jnp.dot(a, b, preferred_element_type=f32)


def slot_hits(routes, experts, capacity):
    top, tokens = routes.shape
    expert = lax.broadcasted_iota(jnp.int32, (experts, tokens), 0)
    hits = [(routes[j : j + 1, :] == expert).astype(f32) for j in range(top)]
    named = functools.reduce(jnp.add, hits).astype(bf16)
    before = lax.broadcasted_iota(jnp.int32, (tokens, tokens), 0)
    after = lax.broadcasted_iota(jnp.int32, (tokens, tokens), 1)
    places = dot(named, (before < after).astype(f32).astype(bf16)).astype(bf16)
    slots = experts * capacity
    first = lax.broadcasted_iota(jnp.int32, (slots, experts), 1) * capacity
    slot = lax.broadcasted_iota(jnp.int32, (slots, experts), 0)
    own = (slot >= first) & (slot < first + capacity)
    spread = own.astype(f32).astype(bf16)
    first_of = jnp.sum(jnp.where(own, first, 0), axis=1, keepdims=True)
    offset = (lax.broadcasted_iota(jnp.int32, (slots, 1), 0) - first_of).astype(f32)
    at_place = dot(spread, places) == offset
    return [(dot(spread, hit.astype(bf16)) > 0.5) & at_place for hit in hits]


def dispatch_kernel(experts, capacity, index, routes, rows, gain, out):
    values = rows[...].astype(f32)
    scale = lax.rsqrt(jnp.mean(values * values, axis=-1, keepdims=True) + eps)
    width = out.shape[1]
    start = pl.multiple_of(index[0] * width, width)
    own = rows[:, pl.ds(start, width)].astype(f32)
    normed = (own * scale * gain[:, pl.ds(start, width)]).astype(bf16)
    matches = slot_hits(routes[...], experts, capacity)
    picker = functools.reduce(jnp.logical_or, matches).astype(f32).astype(bf16)
    out[...] = dot(picker, normed).astype(bf16)


def combiner_kernel(experts, capacity, routes, weights, high, low):
    matches = slot_hits(routes[...], experts, capacity)
    terms = [jnp.where(m, weights[j : j + 1, :], 0.0) for j, m in enumerate(matches)]
    total = functools.reduce(jnp.add, terms).T
    rounded = total.astype(bf16)
    high[...] = rounded
    low[...] = (total - rounded.astype(f32)).astype(bf16)


def combine_kernel(high, low, results, out):
    out[...] = (dot(high[...], results[...]) + dot(low[...], results[...])).astype(bf16)


def experts_kernel(
    index, x_0, x_1, x_3, x_2a, x_2b, gate_0, up_0, down_0, gate_1, up_1, down_1, out, wide, tall, held_out, sems, out_sems
):
    blocks, width = out.shape[0], out.shape[2]
    arriving = (wide.at[0], wide.at[1], tall)
    copies = [
        pltpu.make_async_copy(w.at[0], h, sems.at[i])
        for i, (w, h) in enumerate(zip((gate_1, up_1, down_1), arriving))
    ]
    for copy in copies:
        copy.start()
    depth = x_0.shape[1]
    parts = gate_0.shape[1] // depth
    rows = (x_0[...], x_1[...], jnp.concatenate([x_2a[...], x_2b[...]], axis=0), x_3[...])
    places = [lax.rem(index[0] + k, parts) * depth for k in range(parts)]

    def projected(weight):
        spans = [pl.ds(pl.multiple_of(p, depth), depth) for p in places]
        return functools.reduce(jnp.add, [dot(r, weight[s, :]) for r, s in zip(rows, spans)])

    gate = projected(gate_0.at[0])
    hidden = [(jax.nn.silu(gate) * projected(up_0.at[0])).astype(bf16)]
    copies[0].wait()
    gate = projected(wide.at[0])
    copies[1].wait()
    hidden.append((jax.nn.silu(gate) * projected(wide.at[1])).astype(bf16))
    copies[2].wait()
    stores = []
    for b in range(blocks):
        span = slice(b * width, (b + 1) * width)
        piece = dot(hidden[0], down_0[0, :, span]) + dot(hidden[1], tall[:, span])
        held_out[b] = piece.astype(bf16)
        stores.append(pltpu.make_async_copy(held_out.at[b], out.at[b], out_sems.at[b]))
        stores[-1].start()
    for store in stores:
        store.wait()


def sum_kernel(pieces, out):
    total = pieces[0].astype(f32)
    for b in range(1, pieces.shape[0]):
        total = total + pieces[b].astype(f32)
    out[...] = total.astype(bf16)


def mixer_kernel(index, *refs):
    *pieces, gain, weight, out = refs
    n, width = len(pieces), pieces[0].shape[1]
    values = jnp.concatenate([p[...] for p in pieces], axis=1).astype(f32)
    spans = [
        pl.ds(pl.multiple_of(lax.rem(index[0] + n - k, n) * width, width), width) for k in range(n)
    ]
    gains = jnp.concatenate([gain[:, span] for span in spans], axis=1)
    weights = jnp.concatenate([weight[span, :] for span in spans], axis=0)
    centered = values - jnp.mean(values, axis=-1, keepdims=True)
    scale = lax.rsqrt(jnp.mean(centered * centered, axis=-1, keepdims=True) + eps)
    activated = jax.nn.silu(centered * scale * gains).astype(bf16)
    out[...] = dot(activated, weights).astype(bf16)


def moved(value, by):
    n = lax.axis_size("tp")
    return lax.ppermute(value, "tp", [(i, (i + by) % n) for i in range(n)])


def partner(value):
    return lax.ppermute(value, "core", [(0, 1), (1, 0)])


def params(mib):
    return pltpu.CompilerParams(vmem_limit_bytes=mib << 20)


def cost(flops, moved):
    return pl.CostEstimate(flops=flops, bytes_accessed=moved, transcendentals=0)


def step_on_device(
    value_in,
    gate_in,
    conv_taps,
    chan_gain,
    out_weight,
    second_rows,
    expert_gain,
    routes,
    route_weights,
    gate_w,
    up_w,
    down_w,
):
    n_z, n_core, n_tp = lax.axis_size("z"), lax.axis_size("core"), lax.axis_size("tp")
    experts = n_z
    tokens, width = second_rows.shape
    top = routes.shape[1]
    capacity = 2 * max(1, min(tokens // 2, 3 * tokens * top // (4 * experts)))
    columns = width // n_tp
    slots = experts * capacity
    vmem = pl.BlockSpec(memory_space=pltpu.VMEM)
    smem = pl.BlockSpec(memory_space=pltpu.SMEM)

    routes_t = routes.T
    me = lax.axis_index("tp")
    parts = n_tp // 2
    wide = width // parts
    quarter = lax.rem(me, parts).astype(jnp.int32).reshape(1)
    outgoing = pl.pallas_call(
        functools.partial(dispatch_kernel, experts, capacity),
        grid=(1,),
        out_shape=jax.ShapeDtypeStruct((slots, wide), bf16),
        in_specs=[smem] + [pl.BlockSpec(s, lambda i: (0, 0)) for s in ((top, tokens), (tokens, width), (1, width))],
        out_specs=pl.BlockSpec((slots, wide), lambda i: (0, 0)),
        compiler_params=params(60),
        cost_estimate=cost(10**8, 10**6),
    )(quarter, routes_t, second_rows, expert_gain.reshape(1, -1))
    arrived = lax.all_to_all(
        outgoing.reshape(experts, capacity, wide), "z", split_axis=0, concat_axis=0, tiled=True
    )

    taps = conv_taps.shape[0]
    halo = -(-(taps - 1) // 16) * 16
    glu = (value_in.astype(f32) * jax.nn.sigmoid(gate_in.astype(f32))).astype(bf16)
    length, channels = glu.shape
    n_ep = n_z * n_core
    before = lax.ppermute(
        glu[length - halo :], ("z", "core"), [(i, i + 1) for i in range(n_ep - 1)]
    )
    padded = jnp.concatenate([before, glu], axis=0).astype(f32)
    total = jnp.zeros(glu.shape, f32)
    for offset in range(taps):
        start = halo - taps + 1 + offset
        total = total + conv_taps[offset][None, :] * padded[start : start + length]
    convolved = total.astype(bf16)
    across = moved(convolved, parts)
    from_back = [moved(convolved, k) for k in range(1, parts - 1)]
    from_front = [moved(convolved, -k) for k in range(1, parts - 1)]
    from_back.append(moved(convolved, parts - 1))
    from_front.append(moved(convolved, 1 - parts))

    rows = n_z * capacity
    arrived, _ = lax.optimization_barrier((arrived, convolved))
    x_0 = arrived.reshape(rows, wide)
    x_2a, x_2b = moved(x_0[: rows // 2], -2), moved(x_0[rows // 2 :], 2)
    x_1, x_3 = moved(x_0, -1), moved(x_0, 1)
    gate_b, up_b, down_b = (partner(w) for w in (gate_w, up_w, down_w))
    hbm = pl.BlockSpec(memory_space=pl.ANY)
    units = gate_w.shape[2]
    pieces = pl.pallas_call(
        experts_kernel,
        out_shape=jax.ShapeDtypeStruct((n_tp, rows, columns), bf16),
        in_specs=[smem] + [vmem] * 8 + [hbm] * 3,
        out_specs=hbm,
        scratch_shapes=[
            pltpu.VMEM((2, width, units), bf16),
            pltpu.VMEM((units, width), bf16),
            pltpu.VMEM((n_tp, rows, columns), bf16),
            pltpu.SemaphoreType.DMA((3,)),
            pltpu.SemaphoreType.DMA((n_tp,)),
        ],
        compiler_params=params(24),
        cost_estimate=cost(3 * 10**9, 10**7),
    )(quarter, x_0, x_1, x_3, x_2a, x_2b, gate_w, up_w, down_w, gate_b, up_b, down_b)
    pieces = lax.all_to_all(pieces, "tp", split_axis=0, concat_axis=0, tiled=True)
    step = rows // 2
    sums = pl.pallas_call(
        sum_kernel,
        grid=(rows // step,),
        out_shape=jax.ShapeDtypeStruct((rows, columns), bf16),
        in_specs=[pl.BlockSpec((n_tp, step, columns), lambda i: (0, i, 0))],
        out_specs=pl.BlockSpec((step, columns), lambda i: (i, 0)),
        compiler_params=params(16),
        cost_estimate=cost(10**8, 2 * 10**6),
    )(pieces)
    results = lax.all_to_all(
        sums.reshape(n_z, capacity, columns), "z", split_axis=0, concat_axis=0, tiled=True
    ).reshape(slots, columns)

    high, low = pl.pallas_call(
        functools.partial(combiner_kernel, experts, capacity),
        out_shape=[jax.ShapeDtypeStruct((tokens, slots), bf16)] * 2,
        in_specs=[vmem] * 2,
        out_specs=[vmem] * 2,
        compiler_params=params(16),
        cost_estimate=cost(10**8, 10**6),
    )(routes_t, route_weights.T)
    routed_rows = pl.pallas_call(
        combine_kernel,
        out_shape=jax.ShapeDtypeStruct((tokens, columns), bf16),
        in_specs=[vmem] * 3,
        out_specs=vmem,
        compiler_params=params(16),
        cost_estimate=cost(10**8, 10**6),
    )(high, low, results)
    step = length // 2
    gathered = [convolved, *from_back, across, *from_front[::-1]]
    mixer_rows = pl.pallas_call(
        mixer_kernel,
        grid=(length // step,),
        out_shape=jax.ShapeDtypeStruct((length, out_weight.shape[1]), bf16),
        in_specs=[smem]
        + [pl.BlockSpec((step, channels), lambda i: (i, 0))] * n_tp
        + [
            pl.BlockSpec((1, n_tp * channels), lambda i: (0, 0)),
            pl.BlockSpec(out_weight.shape, lambda i: (0, 0)),
        ],
        out_specs=pl.BlockSpec((step, out_weight.shape[1]), lambda i: (i, 0)),
        compiler_params=params(16),
        cost_estimate=cost(10**9, 2 * 10**6),
    )(me.astype(jnp.int32).reshape(1), *gathered, chan_gain.reshape(1, -1), out_weight)
    return (mixer_rows, routed_rows)


def solution(mesh):
    n_grp, n_ep, n_tp = (mesh.shape[name] for name in ("grp", "ep", "tp"))
    finer = Mesh(mesh.devices.reshape(n_grp, n_ep // 2, 2, n_tp), ("grp", "z", "core", "tp"))
    tok = ("grp", "z", "core")
    placed = (
        P(tok, "tp"),
        P(tok, "tp"),
        P(None, "tp"),
        P(),
        P(None, "tp"),
        P(tok, None),
        P(),
        P(tok, None),
        P(tok, None),
        P(("z", "core"), None, "tp"),
        P(("z", "core"), None, "tp"),
        P(("z", "core"), "tp", None),
    )
    return jax.shard_map(
        step_on_device,
        mesh=finer,
        in_specs=placed,
        out_specs=(P(tok, "tp"), P(tok, "tp")),
        check_vma=False,
    )
```

```python
import functools

import jax
import jax.numpy as jnp
from jax import lax
from jax.experimental import pallas as pl
from jax.experimental.pallas import tpu as pltpu
from jax.sharding import Mesh
from jax.sharding import PartitionSpec as P


eps = 1e-06
f32 = jnp.float32
bf16 = jnp.bfloat16


def dot(a, b):
    return jnp.dot(a, b, preferred_element_type=f32)


def slot_hits(routes, experts, capacity):
    top, tokens = routes.shape
    expert = lax.broadcasted_iota(jnp.int32, (experts, tokens), 0)
    hits = [(routes[j : j + 1, :] == expert).astype(f32) for j in range(top)]
    named = functools.reduce(jnp.add, hits).astype(bf16)
    before = lax.broadcasted_iota(jnp.int32, (tokens, tokens), 0)
    after = lax.broadcasted_iota(jnp.int32, (tokens, tokens), 1)
    places = dot(named, (before < after).astype(f32).astype(bf16))
    place = lax.broadcasted_iota(jnp.int32, (experts, capacity, tokens), 1).astype(f32)
    at_place = places[:, None, :] == place
    slots = experts * capacity
    return [
        jnp.where(at_place, hit[:, None, :], 0.0).reshape(slots, tokens) for hit in hits
    ]


def dispatch_kernel(experts, capacity, index, routes, rows, gain, out):
    values = rows[...].astype(f32)
    scale = lax.rsqrt(jnp.mean(values * values, axis=-1, keepdims=True) + eps)
    width = out.shape[1]
    start = pl.multiple_of(index[0] * width, width)
    own = rows[:, pl.ds(start, width)].astype(f32)
    normed = (own * scale * gain[:, pl.ds(start, width)]).astype(bf16)
    matches = slot_hits(routes[...], experts, capacity)
    picker = functools.reduce(jnp.add, matches).astype(bf16)
    out[...] = dot(picker, normed).astype(bf16)


def combiner_kernel(experts, capacity, routes, weights, high, low):
    matches = slot_hits(routes[...], experts, capacity)
    terms = [m * weights[j : j + 1, :] for j, m in enumerate(matches)]
    total = functools.reduce(jnp.add, terms).T
    rounded = total.astype(bf16)
    high[...] = rounded
    low[...] = (total - rounded.astype(f32)).astype(bf16)


def combine_kernel(high, low, results, out):
    out[...] = (dot(high[...], results[...]) + dot(low[...], results[...])).astype(bf16)


def experts_kernel(
    index, x_0, x_1, x_3, x_2a, x_2b, gate_0, up_0, gate_1, up_1, down_1, down_0, out, tall, held_out, sem, out_sems
):
    blocks, width = out.shape[0], out.shape[2]
    load = pltpu.make_async_copy(down_0.at[0], tall, sem)
    load.start()
    depth = x_0.shape[1]
    parts = gate_0.shape[1] // depth
    rows = (x_0[...], x_1[...], jnp.concatenate([x_2a[...], x_2b[...]], axis=0), x_3[...])
    places = [lax.rem(index[0] + k, parts) * depth for k in range(parts)]

    def projected(weight):
        spans = [pl.ds(pl.multiple_of(p, depth), depth) for p in places]
        return functools.reduce(jnp.add, [dot(r, weight[0, s, :]) for r, s in zip(rows, spans)])

    hidden = [
        (jax.nn.silu(projected(g)) * projected(u)).astype(bf16)
        for g, u in ((gate_0, up_0), (gate_1, up_1))
    ]
    load.wait()
    stores = []
    for b in range(blocks):
        span = slice(b * width, (b + 1) * width)
        piece = dot(hidden[0], tall[:, span]) + dot(hidden[1], down_1[0, :, span])
        held_out[b] = piece.astype(bf16)
        stores.append(pltpu.make_async_copy(held_out.at[b], out.at[b], out_sems.at[b]))
        stores[-1].start()
    for store in stores:
        store.wait()


def sum_kernel(pieces, out):
    total = pieces[0].astype(f32)
    for b in range(1, pieces.shape[0]):
        total = total + pieces[b].astype(f32)
    out[...] = total.astype(bf16)


def mixer_kernel(index, *refs):
    *pieces, gain, weight, out = refs
    n, width = len(pieces), pieces[0].shape[1]
    values = jnp.concatenate([p[...] for p in pieces], axis=1).astype(f32)
    spans = [
        pl.ds(pl.multiple_of(lax.rem(index[0] + n - k, n) * width, width), width) for k in range(n)
    ]
    gains = jnp.concatenate([gain[:, span] for span in spans], axis=1)
    weights = jnp.concatenate([weight[span, :] for span in spans], axis=0)
    centered = values - jnp.mean(values, axis=-1, keepdims=True)
    scale = lax.rsqrt(jnp.mean(centered * centered, axis=-1, keepdims=True) + eps)
    activated = jax.nn.silu(centered * scale * gains).astype(bf16)
    out[...] = dot(activated, weights).astype(bf16)


def moved(value, by):
    n = lax.axis_size("tp")
    return lax.ppermute(value, "tp", [(i, (i + by) % n) for i in range(n)])


def partner(value):
    return lax.ppermute(value, "core", [(0, 1), (1, 0)])


def params(mib):
    return pltpu.CompilerParams(vmem_limit_bytes=mib << 20)


def cost(flops, moved):
    return pl.CostEstimate(flops=flops, bytes_accessed=moved, transcendentals=0)


def step_on_device(
    value_in,
    gate_in,
    conv_taps,
    chan_gain,
    out_weight,
    second_rows,
    expert_gain,
    routes,
    route_weights,
    gate_w,
    up_w,
    down_w,
):
    n_z, n_core, n_tp = lax.axis_size("z"), lax.axis_size("core"), lax.axis_size("tp")
    experts = n_z
    tokens, width = second_rows.shape
    top = routes.shape[1]
    capacity = 2 * max(1, min(tokens // 2, 3 * tokens * top // (4 * experts)))
    columns = width // n_tp
    slots = experts * capacity
    vmem = pl.BlockSpec(memory_space=pltpu.VMEM)
    smem = pl.BlockSpec(memory_space=pltpu.SMEM)

    routes_t = routes.T
    me = lax.axis_index("tp")
    parts = n_tp // 2
    wide = width // parts
    quarter = lax.rem(me, parts).astype(jnp.int32).reshape(1)
    outgoing = pl.pallas_call(
        functools.partial(dispatch_kernel, experts, capacity),
        grid=(1,),
        out_shape=jax.ShapeDtypeStruct((slots, wide), bf16),
        in_specs=[smem] + [pl.BlockSpec(s, lambda i: (0, 0)) for s in ((top, tokens), (tokens, width), (1, width))],
        out_specs=pl.BlockSpec((slots, wide), lambda i: (0, 0)),
        compiler_params=params(60),
        cost_estimate=cost(10**8, 10**6),
    )(quarter, routes_t, second_rows, expert_gain.reshape(1, -1))
    arrived = lax.all_to_all(
        outgoing.reshape(experts, capacity, wide), "z", split_axis=0, concat_axis=0, tiled=True
    )

    taps = conv_taps.shape[0]
    halo = -(-(taps - 1) // 16) * 16
    glu = (value_in.astype(f32) * jax.nn.sigmoid(gate_in.astype(f32))).astype(bf16)
    length, channels = glu.shape
    n_ep = n_z * n_core
    before = lax.ppermute(
        glu[length - halo :], ("z", "core"), [(i, i + 1) for i in range(n_ep - 1)]
    )
    padded = jnp.concatenate([before, glu], axis=0).astype(f32)
    total = jnp.zeros(glu.shape, f32)
    for offset in range(taps):
        start = halo - taps + 1 + offset
        total = total + conv_taps[offset][None, :] * padded[start : start + length]
    convolved = total.astype(bf16)
    across = moved(convolved, parts)
    from_back = [moved(convolved, k) for k in range(1, parts - 1)]
    from_front = [moved(convolved, -k) for k in range(1, parts - 1)]
    from_back.append(moved(convolved, parts - 1))
    from_front.append(moved(convolved, 1 - parts))

    rows = n_z * capacity
    arrived, _ = lax.optimization_barrier((arrived, convolved))
    x_0 = arrived.reshape(rows, wide)
    x_2a, x_2b = moved(x_0[: rows // 2], -2), moved(x_0[rows // 2 :], 2)
    x_1, x_3 = moved(x_0, -1), moved(x_0, 1)
    gate_b, up_b, down_b = (partner(w) for w in (gate_w, up_w, down_w))
    hbm = pl.BlockSpec(memory_space=pl.ANY)
    units = gate_w.shape[2]
    pieces = pl.pallas_call(
        experts_kernel,
        out_shape=jax.ShapeDtypeStruct((n_tp, rows, columns), bf16),
        in_specs=[smem] + [vmem] * 10 + [pl.BlockSpec(memory_space=pltpu.HBM)],
        out_specs=hbm,
        scratch_shapes=[
            pltpu.VMEM((units, width), bf16),
            pltpu.VMEM((n_tp, rows, columns), bf16),
            pltpu.SemaphoreType.DMA,
            pltpu.SemaphoreType.DMA((n_tp,)),
        ],
        compiler_params=params(24),
        cost_estimate=cost(3 * 10**9, 10**7),
    )(quarter, x_0, x_1, x_3, x_2a, x_2b, gate_w, up_w, gate_b, up_b, down_b, down_w)
    pieces = lax.all_to_all(pieces, "tp", split_axis=0, concat_axis=0, tiled=True)
    step = rows // 2
    sums = pl.pallas_call(
        sum_kernel,
        grid=(rows // step,),
        out_shape=jax.ShapeDtypeStruct((rows, columns), bf16),
        in_specs=[pl.BlockSpec((n_tp, step, columns), lambda i: (0, i, 0))],
        out_specs=pl.BlockSpec((step, columns), lambda i: (i, 0)),
        compiler_params=params(16),
        cost_estimate=cost(10**8, 2 * 10**6),
    )(pieces)
    results = lax.all_to_all(
        sums.reshape(n_z, capacity, columns), "z", split_axis=0, concat_axis=0, tiled=True
    ).reshape(slots, columns)

    high, low = pl.pallas_call(
        functools.partial(combiner_kernel, experts, capacity),
        out_shape=[jax.ShapeDtypeStruct((tokens, slots), bf16)] * 2,
        in_specs=[vmem] * 2,
        out_specs=[vmem] * 2,
        compiler_params=params(16),
        cost_estimate=cost(10**8, 10**6),
    )(routes_t, route_weights.T)
    routed_rows = pl.pallas_call(
        combine_kernel,
        out_shape=jax.ShapeDtypeStruct((tokens, columns), bf16),
        in_specs=[vmem] * 3,
        out_specs=vmem,
        compiler_params=params(16),
        cost_estimate=cost(10**8, 10**6),
    )(high, low, results)
    routed_rows, from_back = lax.optimization_barrier((routed_rows, from_back))
    step = length // 2
    gathered = [convolved, *from_back, across, *from_front[::-1]]
    mixer_rows = pl.pallas_call(
        mixer_kernel,
        grid=(length // step,),
        out_shape=jax.ShapeDtypeStruct((length, out_weight.shape[1]), bf16),
        in_specs=[smem]
        + [pl.BlockSpec((step, channels), lambda i: (i, 0))] * n_tp
        + [
            pl.BlockSpec((1, n_tp * channels), lambda i: (0, 0)),
            pl.BlockSpec(out_weight.shape, lambda i: (0, 0)),
        ],
        out_specs=pl.BlockSpec((step, out_weight.shape[1]), lambda i: (i, 0)),
        compiler_params=params(16),
        cost_estimate=cost(10**9, 2 * 10**6),
    )(me.astype(jnp.int32).reshape(1), *gathered, chan_gain.reshape(1, -1), out_weight)
    return (mixer_rows, routed_rows)


def solution(mesh):
    n_grp, n_ep, n_tp = (mesh.shape[name] for name in ("grp", "ep", "tp"))
    finer = Mesh(mesh.devices.reshape(n_grp, n_ep // 2, 2, n_tp), ("grp", "z", "core", "tp"))
    tok = ("grp", "z", "core")
    placed = (
        P(tok, "tp"),
        P(tok, "tp"),
        P(None, "tp"),
        P(),
        P(None, "tp"),
        P(tok, None),
        P(),
        P(tok, None),
        P(tok, None),
        P(("z", "core"), None, "tp"),
        P(("z", "core"), None, "tp"),
        P(("z", "core"), "tp", None),
    )
    return jax.shard_map(
        step_on_device,
        mesh=finer,
        in_specs=placed,
        out_specs=(P(tok, "tp"), P(tok, "tp")),
        check_vma=False,
    )
```

```python
import functools

import jax
import jax.numpy as jnp
from jax import lax
from jax.experimental import pallas as pl
from jax.experimental.pallas import tpu as pltpu
from jax.sharding import Mesh
from jax.sharding import PartitionSpec as P


eps = 1e-06
f32 = jnp.float32
bf16 = jnp.bfloat16


def dot(a, b):
    return jnp.dot(a, b, preferred_element_type=f32)


def slot_hits(routes, experts, capacity):
    top, tokens = routes.shape
    expert = lax.broadcasted_iota(jnp.int32, (experts, tokens), 0)
    hits = [(routes[j : j + 1, :] == expert).astype(f32) for j in range(top)]
    named = functools.reduce(jnp.add, hits).astype(bf16)
    before = lax.broadcasted_iota(jnp.int32, (tokens, tokens), 0)
    after = lax.broadcasted_iota(jnp.int32, (tokens, tokens), 1)
    places = dot(named, (before < after).astype(f32).astype(bf16))
    place = lax.broadcasted_iota(jnp.int32, (experts, capacity, tokens), 1).astype(f32)
    at_place = places[:, None, :] == place
    slots = experts * capacity
    return [
        jnp.where(at_place, hit[:, None, :], 0.0).reshape(slots, tokens) for hit in hits
    ]


def dispatch_kernel(experts, capacity, index, routes, rows, gain, out):
    values = rows[...].astype(f32)
    scale = lax.rsqrt(jnp.mean(values * values, axis=-1, keepdims=True) + eps)
    width = out.shape[1]
    start = pl.multiple_of(index[0] * width, width)
    own = rows[:, pl.ds(start, width)].astype(f32)
    normed = (own * scale * gain[:, pl.ds(start, width)]).astype(bf16)
    matches = slot_hits(routes[...], experts, capacity)
    picker = functools.reduce(jnp.add, matches).astype(bf16)
    out[...] = dot(picker, normed).astype(bf16)


def combiner_kernel(experts, capacity, routes, weights, high, low):
    matches = slot_hits(routes[...], experts, capacity)
    terms = [m * weights[j : j + 1, :] for j, m in enumerate(matches)]
    total = functools.reduce(jnp.add, terms).T
    rounded = total.astype(bf16)
    high[...] = rounded
    low[...] = (total - rounded.astype(f32)).astype(bf16)


def combine_kernel(high, low, results, out):
    out[...] = (dot(high[...], results[...]) + dot(low[...], results[...])).astype(bf16)


def experts_kernel(
    index, x_0, x_1, x_3, x_2a, x_2b, gate_0, up_0, gate_1, up_1, down_0, down_1, out, tall, sem
):
    blocks, width = out.shape[0], out.shape[2]
    load = pltpu.make_async_copy(down_1.at[0], tall, sem)
    load.start()
    depth = x_0.shape[1]
    parts = gate_0.shape[1] // depth
    rows = (x_0[...], x_1[...], jnp.concatenate([x_2a[...], x_2b[...]], axis=0), x_3[...])
    places = [lax.rem(index[0] + k, parts) * depth for k in range(parts)]

    def projected(weight):
        spans = [pl.ds(pl.multiple_of(p, depth), depth) for p in places]
        return functools.reduce(jnp.add, [dot(r, weight[0, s, :]) for r, s in zip(rows, spans)])

    hidden = [
        (jax.nn.silu(projected(g)) * projected(u)).astype(bf16)
        for g, u in ((gate_0, up_0), (gate_1, up_1))
    ]
    load.wait()
    for b in range(blocks):
        span = slice(b * width, (b + 1) * width)
        piece = dot(hidden[0], down_0[0, :, span]) + dot(hidden[1], tall[:, span])
        out[b] = piece.astype(bf16)


def sum_kernel(pieces, out):
    total = pieces[0].astype(f32)
    for b in range(1, pieces.shape[0]):
        total = total + pieces[b].astype(f32)
    out[...] = total.astype(bf16)


def mixer_kernel(index, *refs):
    *pieces, gain, weight, out = refs
    n, width = len(pieces), pieces[0].shape[1]
    values = jnp.concatenate([p[...] for p in pieces], axis=1).astype(f32)
    spans = [
        pl.ds(pl.multiple_of(lax.rem(index[0] + n - k, n) * width, width), width) for k in range(n)
    ]
    gains = jnp.concatenate([gain[:, span] for span in spans], axis=1)
    weights = jnp.concatenate([weight[span, :] for span in spans], axis=0)
    centered = values - jnp.mean(values, axis=-1, keepdims=True)
    scale = lax.rsqrt(jnp.mean(centered * centered, axis=-1, keepdims=True) + eps)
    activated = jax.nn.silu(centered * scale * gains).astype(bf16)
    out[...] = dot(activated, weights).astype(bf16)


def moved(value, by):
    n = lax.axis_size("tp")
    return lax.ppermute(value, "tp", [(i, (i + by) % n) for i in range(n)])


def partner(value):
    return lax.ppermute(value, "core", [(0, 1), (1, 0)])


def params(mib):
    return pltpu.CompilerParams(vmem_limit_bytes=mib << 20)


def cost(flops, moved):
    return pl.CostEstimate(flops=flops, bytes_accessed=moved, transcendentals=0)


def step_on_device(
    value_in,
    gate_in,
    conv_taps,
    chan_gain,
    out_weight,
    second_rows,
    expert_gain,
    routes,
    route_weights,
    gate_w,
    up_w,
    down_w,
):
    n_z, n_core, n_tp = lax.axis_size("z"), lax.axis_size("core"), lax.axis_size("tp")
    experts = n_z
    tokens, width = second_rows.shape
    top = routes.shape[1]
    capacity = 2 * max(1, min(tokens // 2, 3 * tokens * top // (4 * experts)))
    columns = width // n_tp
    slots = experts * capacity
    vmem = pl.BlockSpec(memory_space=pltpu.VMEM)
    smem = pl.BlockSpec(memory_space=pltpu.SMEM)

    routes_t = routes.T
    me = lax.axis_index("tp")
    parts = n_tp // 2
    wide = width // parts
    quarter = lax.rem(me, parts).astype(jnp.int32).reshape(1)
    outgoing = pl.pallas_call(
        functools.partial(dispatch_kernel, experts, capacity),
        grid=(1,),
        out_shape=jax.ShapeDtypeStruct((slots, wide), bf16),
        in_specs=[smem] + [pl.BlockSpec(s, lambda i: (0, 0)) for s in ((top, tokens), (tokens, width), (1, width))],
        out_specs=pl.BlockSpec((slots, wide), lambda i: (0, 0)),
        compiler_params=params(60),
        cost_estimate=cost(10**8, 10**6),
    )(quarter, routes_t, second_rows, expert_gain.reshape(1, -1))
    arrived = lax.all_to_all(
        outgoing.reshape(experts, capacity, wide), "z", split_axis=0, concat_axis=0, tiled=True
    )

    taps = conv_taps.shape[0]
    halo = -(-(taps - 1) // 16) * 16
    glu = (value_in.astype(f32) * jax.nn.sigmoid(gate_in.astype(f32))).astype(bf16)
    length, channels = glu.shape
    n_ep = n_z * n_core
    before = lax.ppermute(
        glu[length - halo :], ("z", "core"), [(i, i + 1) for i in range(n_ep - 1)]
    )
    padded = jnp.concatenate([before, glu], axis=0).astype(f32)
    total = jnp.zeros(glu.shape, f32)
    for offset in range(taps):
        start = halo - taps + 1 + offset
        total = total + conv_taps[offset][None, :] * padded[start : start + length]
    convolved = total.astype(bf16)
    from_back, from_front = {}, {}
    for k in range(parts, 0, -1):
        from_back[k] = moved(convolved, k)
        if k < parts:
            from_front[k] = moved(convolved, -k)

    rows = n_z * capacity
    arrived, _ = lax.optimization_barrier((arrived, convolved))
    x_0 = arrived.reshape(rows, wide)
    x_2a, x_2b = moved(x_0[: rows // 2], -2), moved(x_0[rows // 2 :], 2)
    x_1, x_3 = moved(x_0, -1), moved(x_0, 1)
    down_b = partner(down_w)
    gate_b, up_b = partner(gate_w), partner(up_w)
    units = gate_w.shape[2]
    pieces = pl.pallas_call(
        experts_kernel,
        out_shape=jax.ShapeDtypeStruct((n_tp, rows, columns), bf16),
        in_specs=[smem] + [vmem] * 10 + [pl.BlockSpec(memory_space=pl.ANY)],
        out_specs=vmem,
        scratch_shapes=[pltpu.VMEM((units, width), bf16), pltpu.SemaphoreType.DMA],
        compiler_params=params(24),
        cost_estimate=cost(3 * 10**9, 10**7),
    )(quarter, x_0, x_1, x_3, x_2a, x_2b, gate_w, up_w, gate_b, up_b, down_w, down_b)
    pieces = lax.all_to_all(pieces, "tp", split_axis=0, concat_axis=0, tiled=True)
    step = rows // 2
    sums = pl.pallas_call(
        sum_kernel,
        grid=(rows // step,),
        out_shape=jax.ShapeDtypeStruct((rows, columns), bf16),
        in_specs=[pl.BlockSpec((n_tp, step, columns), lambda i: (0, i, 0))],
        out_specs=pl.BlockSpec((step, columns), lambda i: (i, 0)),
        compiler_params=params(16),
        cost_estimate=cost(10**8, 2 * 10**6),
    )(pieces)
    results = lax.all_to_all(
        sums.reshape(n_z, capacity, columns), "z", split_axis=0, concat_axis=0, tiled=True
    ).reshape(slots, columns)

    high, low = pl.pallas_call(
        functools.partial(combiner_kernel, experts, capacity),
        out_shape=[jax.ShapeDtypeStruct((tokens, slots), bf16)] * 2,
        in_specs=[vmem] * 2,
        out_specs=[vmem] * 2,
        compiler_params=params(16),
        cost_estimate=cost(10**8, 10**6),
    )(routes_t, route_weights.T)
    routed_rows = pl.pallas_call(
        combine_kernel,
        out_shape=jax.ShapeDtypeStruct((tokens, columns), bf16),
        in_specs=[vmem] * 3,
        out_specs=vmem,
        compiler_params=params(16),
        cost_estimate=cost(10**8, 10**6),
    )(high, low, results)
    step = length // 2
    gathered = [convolved] + [from_back[k] for k in range(1, parts + 1)]
    gathered += [from_front[k] for k in range(parts - 1, 0, -1)]
    mixer_rows = pl.pallas_call(
        mixer_kernel,
        grid=(length // step,),
        out_shape=jax.ShapeDtypeStruct((length, out_weight.shape[1]), bf16),
        in_specs=[smem]
        + [pl.BlockSpec((step, channels), lambda i: (i, 0))] * n_tp
        + [
            pl.BlockSpec((1, n_tp * channels), lambda i: (0, 0)),
            pl.BlockSpec(out_weight.shape, lambda i: (0, 0)),
        ],
        out_specs=pl.BlockSpec((step, out_weight.shape[1]), lambda i: (i, 0)),
        compiler_params=params(16),
        cost_estimate=cost(10**9, 2 * 10**6),
    )(me.astype(jnp.int32).reshape(1), *gathered, chan_gain.reshape(1, -1), out_weight)
    return (mixer_rows, routed_rows)


def solution(mesh):
    n_grp, n_ep, n_tp = (mesh.shape[name] for name in ("grp", "ep", "tp"))
    finer = Mesh(mesh.devices.reshape(n_grp, n_ep // 2, 2, n_tp), ("grp", "z", "core", "tp"))
    tok = ("grp", "z", "core")
    placed = (
        P(tok, "tp"),
        P(tok, "tp"),
        P(None, "tp"),
        P(),
        P(None, "tp"),
        P(tok, None),
        P(),
        P(tok, None),
        P(tok, None),
        P(("z", "core"), None, "tp"),
        P(("z", "core"), None, "tp"),
        P(("z", "core"), "tp", None),
    )
    return jax.shard_map(
        step_on_device,
        mesh=finer,
        in_specs=placed,
        out_specs=(P(tok, "tp"), P(tok, "tp")),
        check_vma=False,
    )
```

```python
import functools

import jax
import jax.numpy as jnp
from jax import lax
from jax.experimental import pallas as pl
from jax.experimental.pallas import tpu as pltpu
from jax.sharding import Mesh
from jax.sharding import PartitionSpec as P


eps = 1e-06
f32 = jnp.float32
bf16 = jnp.bfloat16


def dot(a, b):
    return jnp.dot(a, b, preferred_element_type=f32)


def slot_hits(routes, experts, capacity):
    top, tokens = routes.shape
    expert = lax.broadcasted_iota(jnp.int32, (experts, tokens), 0)
    hits = [(routes[j : j + 1, :] == expert).astype(f32) for j in range(top)]
    named = functools.reduce(jnp.add, hits).astype(bf16)
    before = lax.broadcasted_iota(jnp.int32, (tokens, tokens), 0)
    after = lax.broadcasted_iota(jnp.int32, (tokens, tokens), 1)
    places = dot(named, (before < after).astype(f32).astype(bf16))
    place = lax.broadcasted_iota(jnp.int32, (experts, capacity, tokens), 1).astype(f32)
    at_place = places[:, None, :] == place
    slots = experts * capacity
    return [
        jnp.where(at_place, hit[:, None, :], 0.0).reshape(slots, tokens) for hit in hits
    ]


def dispatch_kernel(experts, capacity, index, routes, rows, gain, out):
    values = rows[...].astype(f32)
    scale = lax.rsqrt(jnp.mean(values * values, axis=-1, keepdims=True) + eps)
    width = out.shape[1]
    start = pl.multiple_of(index[0] * width, width)
    own = rows[:, pl.ds(start, width)].astype(f32)
    normed = (own * scale * gain[:, pl.ds(start, width)]).astype(bf16)
    matches = slot_hits(routes[...], experts, capacity)
    picker = functools.reduce(jnp.add, matches).astype(bf16)
    out[...] = dot(picker, normed).astype(bf16)


def combiner_kernel(experts, capacity, routes, weights, high, low):
    matches = slot_hits(routes[...], experts, capacity)
    terms = [m * weights[j : j + 1, :] for j, m in enumerate(matches)]
    total = functools.reduce(jnp.add, terms).T
    rounded = total.astype(bf16)
    high[...] = rounded
    low[...] = (total - rounded.astype(f32)).astype(bf16)


def combine_kernel(high, low, results, out):
    out[...] = (dot(high[...], results[...]) + dot(low[...], results[...])).astype(bf16)


def experts_kernel(
    index, x_0, x_1, x_3, x_2a, x_2b, gate_0, up_0, gate_1, up_1, down_0, down_1, me, out, top, bottom, tall, sem
):
    load = pltpu.make_async_copy(down_1.at[0], tall, sem)
    load.start()
    depth = x_0.shape[1]
    parts = gate_0.shape[1] // depth
    rows = (x_0[...], x_1[...], jnp.concatenate([x_2a[...], x_2b[...]], axis=0), x_3[...])
    places = [lax.rem(index[0] + k, parts) * depth for k in range(parts)]

    def projected(weight):
        spans = [pl.ds(pl.multiple_of(p, depth), depth) for p in places]
        return functools.reduce(jnp.add, [dot(r, weight[0, s, :]) for r, s in zip(rows, spans)])

    hidden = [
        (jax.nn.silu(projected(g)) * projected(u)).astype(bf16)
        for g, u in ((gate_0, up_0), (gate_1, up_1))
    ]
    load.wait()
    half, width = top.shape
    n = tall.shape[1] // width
    span = block_of(me, n // 2, n, width)
    piece = dot(hidden[0], down_0[0, :, span]) + dot(hidden[1], tall[:, span])
    top[...] = piece[:half].astype(bf16)
    bottom[...] = piece[half:].astype(bf16)
    units = hidden[0].shape[1]
    out[:, :units] = hidden[0]
    out[:, units:] = hidden[1]


def block_of(me, by, n, width):
    return pl.ds(pl.multiple_of(lax.rem(me[0] + by + n, n) * width, width), width)


def pieces_kernel(far, me, hidden, down_0, down_1, top, bottom, *outs):
    half, width = top.shape
    n, units = down_1.shape[1] // width, down_1.shape[0]
    order = [0] + [sign * k for k in range(1, far + 1) for sign in (1, -1)]
    for by, out in zip(order, outs):
        span = block_of(me, by, n, width)
        piece = dot(hidden[:, :units], down_0[0, :, span])
        piece = piece + dot(hidden[:, units:], down_1[:, span])
        if by == far:
            piece = jnp.concatenate([piece[:half] + top[...].astype(f32), piece[half:]], axis=0)
        if by == -far:
            piece = jnp.concatenate([piece[:half], piece[half:] + bottom[...].astype(f32)], axis=0)
        out[...] = piece.astype(bf16)


def sum_kernel(*refs):
    *pieces, out = refs
    out[...] = functools.reduce(jnp.add, [p[...].astype(f32) for p in pieces]).astype(bf16)


def mixer_kernel(index, *refs):
    *pieces, gain, weight, out = refs
    n, width = len(pieces), pieces[0].shape[1]
    values = jnp.concatenate([p[...] for p in pieces], axis=1).astype(f32)
    spans = [
        pl.ds(pl.multiple_of(lax.rem(index[0] + n - k, n) * width, width), width) for k in range(n)
    ]
    gains = jnp.concatenate([gain[:, span] for span in spans], axis=1)
    weights = jnp.concatenate([weight[span, :] for span in spans], axis=0)
    centered = values - jnp.mean(values, axis=-1, keepdims=True)
    scale = lax.rsqrt(jnp.mean(centered * centered, axis=-1, keepdims=True) + eps)
    activated = jax.nn.silu(centered * scale * gains).astype(bf16)
    out[...] = dot(activated, weights).astype(bf16)


def moved(value, by):
    n = lax.axis_size("tp")
    return lax.ppermute(value, "tp", [(i, (i + by) % n) for i in range(n)])


def partner(value):
    return lax.ppermute(value, "core", [(0, 1), (1, 0)])


def params(mib):
    return pltpu.CompilerParams(vmem_limit_bytes=mib << 20)


def cost(flops, moved):
    return pl.CostEstimate(flops=flops, bytes_accessed=moved, transcendentals=0)


def step_on_device(
    value_in,
    gate_in,
    conv_taps,
    chan_gain,
    out_weight,
    second_rows,
    expert_gain,
    routes,
    route_weights,
    gate_w,
    up_w,
    down_w,
):
    n_z, n_core, n_tp = lax.axis_size("z"), lax.axis_size("core"), lax.axis_size("tp")
    experts = n_z
    tokens, width = second_rows.shape
    top = routes.shape[1]
    capacity = 2 * max(1, min(tokens // 2, 3 * tokens * top // (4 * experts)))
    columns = width // n_tp
    slots = experts * capacity
    vmem = pl.BlockSpec(memory_space=pltpu.VMEM)
    smem = pl.BlockSpec(memory_space=pltpu.SMEM)

    routes_t = routes.T
    me = lax.axis_index("tp")
    parts = n_tp // 2
    wide = width // parts
    quarter = lax.rem(me, parts).astype(jnp.int32).reshape(1)
    outgoing = pl.pallas_call(
        functools.partial(dispatch_kernel, experts, capacity),
        grid=(1,),
        out_shape=jax.ShapeDtypeStruct((slots, wide), bf16),
        in_specs=[smem] + [pl.BlockSpec(s, lambda i: (0, 0)) for s in ((top, tokens), (tokens, width), (1, width))],
        out_specs=pl.BlockSpec((slots, wide), lambda i: (0, 0)),
        compiler_params=params(60),
        cost_estimate=cost(10**8, 10**6),
    )(quarter, routes_t, second_rows, expert_gain.reshape(1, -1))
    arrived = lax.all_to_all(
        outgoing.reshape(experts, capacity, wide), "z", split_axis=0, concat_axis=0, tiled=True
    )

    taps = conv_taps.shape[0]
    halo = -(-(taps - 1) // 16) * 16
    glu = (value_in.astype(f32) * jax.nn.sigmoid(gate_in.astype(f32))).astype(bf16)
    length, channels = glu.shape
    n_ep = n_z * n_core
    before = lax.ppermute(
        glu[length - halo :], ("z", "core"), [(i, i + 1) for i in range(n_ep - 1)]
    )
    padded = jnp.concatenate([before, glu], axis=0).astype(f32)
    total = jnp.zeros(glu.shape, f32)
    for offset in range(taps):
        start = halo - taps + 1 + offset
        total = total + conv_taps[offset][None, :] * padded[start : start + length]
    convolved = total.astype(bf16)
    from_back, from_front = {}, {}
    for k in range(parts, 0, -1):
        from_back[k] = moved(convolved, k)
        if k < parts:
            from_front[k] = moved(convolved, -k)

    rows = n_z * capacity
    arrived, _ = lax.optimization_barrier((arrived, convolved))
    x_0 = arrived.reshape(rows, wide)
    x_2a, x_2b = moved(x_0[: rows // 2], -2), moved(x_0[rows // 2 :], 2)
    x_1, x_3 = moved(x_0, -1), moved(x_0, 1)
    down_b = partner(down_w)
    gate_b, up_b = partner(gate_w), partner(up_w)
    units = gate_w.shape[2]
    me_ref = me.astype(jnp.int32).reshape(1)
    shape = lambda *dims: jax.ShapeDtypeStruct(dims, bf16)
    hidden, top, bottom, down_b = pl.pallas_call(
        experts_kernel,
        out_shape=[
            shape(rows, 2 * units),
            shape(rows // 2, columns),
            shape(rows // 2, columns),
            shape(units, width),
        ],
        in_specs=[smem] + [vmem] * 10 + [pl.BlockSpec(memory_space=pl.ANY), smem],
        out_specs=[vmem] * 4,
        scratch_shapes=[pltpu.SemaphoreType.DMA],
        compiler_params=params(24),
        cost_estimate=cost(2 * 10**9, 10**7),
    )(quarter, x_0, x_1, x_3, x_2a, x_2b, gate_w, up_w, gate_b, up_b, down_w, down_b, me_ref)
    top, bottom = moved(top, 1), moved(bottom, -1)
    far = parts - 1
    own, *sent = pl.pallas_call(
        functools.partial(pieces_kernel, far),
        out_shape=[shape(rows, columns)] * (2 * far + 1),
        in_specs=[smem] + [vmem] * 5,
        out_specs=[vmem] * (2 * far + 1),
        compiler_params=params(16),
        cost_estimate=cost(10**9, 10**6),
    )(me_ref, hidden, down_w, down_b, top, bottom)
    pieces = [own]
    for k in range(far, 0, -1):
        pieces += [moved(sent[2 * k - 2], k), moved(sent[2 * k - 1], -k)]
    sums = pl.pallas_call(
        sum_kernel,
        out_shape=shape(rows, columns),
        in_specs=[vmem] * len(pieces),
        out_specs=vmem,
        compiler_params=params(16),
        cost_estimate=cost(10**8, 2 * 10**6),
    )(*pieces)
    results = lax.all_to_all(
        sums.reshape(n_z, capacity, columns), "z", split_axis=0, concat_axis=0, tiled=True
    ).reshape(slots, columns)

    high, low = pl.pallas_call(
        functools.partial(combiner_kernel, experts, capacity),
        out_shape=[jax.ShapeDtypeStruct((tokens, slots), bf16)] * 2,
        in_specs=[vmem] * 2,
        out_specs=[vmem] * 2,
        compiler_params=params(16),
        cost_estimate=cost(10**8, 10**6),
    )(routes_t, route_weights.T)
    routed_rows = pl.pallas_call(
        combine_kernel,
        out_shape=jax.ShapeDtypeStruct((tokens, columns), bf16),
        in_specs=[vmem] * 3,
        out_specs=vmem,
        compiler_params=params(16),
        cost_estimate=cost(10**8, 10**6),
    )(high, low, results)
    step = length // 2
    gathered = [convolved] + [from_back[k] for k in range(1, parts + 1)]
    gathered += [from_front[k] for k in range(parts - 1, 0, -1)]
    mixer_rows = pl.pallas_call(
        mixer_kernel,
        grid=(length // step,),
        out_shape=jax.ShapeDtypeStruct((length, out_weight.shape[1]), bf16),
        in_specs=[smem]
        + [pl.BlockSpec((step, channels), lambda i: (i, 0))] * n_tp
        + [
            pl.BlockSpec((1, n_tp * channels), lambda i: (0, 0)),
            pl.BlockSpec(out_weight.shape, lambda i: (0, 0)),
        ],
        out_specs=pl.BlockSpec((step, out_weight.shape[1]), lambda i: (i, 0)),
        compiler_params=params(16),
        cost_estimate=cost(10**9, 2 * 10**6),
    )(me.astype(jnp.int32).reshape(1), *gathered, chan_gain.reshape(1, -1), out_weight)
    return (mixer_rows, routed_rows)


def solution(mesh):
    n_grp, n_ep, n_tp = (mesh.shape[name] for name in ("grp", "ep", "tp"))
    finer = Mesh(mesh.devices.reshape(n_grp, n_ep // 2, 2, n_tp), ("grp", "z", "core", "tp"))
    tok = ("grp", "z", "core")
    placed = (
        P(tok, "tp"),
        P(tok, "tp"),
        P(None, "tp"),
        P(),
        P(None, "tp"),
        P(tok, None),
        P(),
        P(tok, None),
        P(tok, None),
        P(("z", "core"), None, "tp"),
        P(("z", "core"), None, "tp"),
        P(("z", "core"), "tp", None),
    )
    return jax.shard_map(
        step_on_device,
        mesh=finer,
        in_specs=placed,
        out_specs=(P(tok, "tp"), P(tok, "tp")),
        check_vma=False,
    )
```

```python
import functools

import jax
import jax.numpy as jnp
from jax import lax
from jax.experimental import pallas as pl
from jax.experimental.pallas import tpu as pltpu
from jax.sharding import Mesh
from jax.sharding import PartitionSpec as P


eps = 1e-06
f32 = jnp.float32
bf16 = jnp.bfloat16


def dot(a, b):
    return jnp.dot(a, b, preferred_element_type=f32)


def slot_hits(routes, experts, capacity):
    top, tokens = routes.shape
    expert = lax.broadcasted_iota(jnp.int32, (experts, tokens), 0)
    hits = [(routes[j : j + 1, :] == expert).astype(f32) for j in range(top)]
    named = functools.reduce(jnp.add, hits).astype(bf16)
    before = lax.broadcasted_iota(jnp.int32, (tokens, tokens), 0)
    after = lax.broadcasted_iota(jnp.int32, (tokens, tokens), 1)
    places = dot(named, (before < after).astype(f32).astype(bf16))
    place = lax.broadcasted_iota(jnp.int32, (experts, capacity, tokens), 1).astype(f32)
    at_place = places[:, None, :] == place
    slots = experts * capacity
    return [
        jnp.where(at_place, hit[:, None, :], 0.0).reshape(slots, tokens) for hit in hits
    ]


def dispatch_kernel(experts, capacity, index, routes, rows, gain, out):
    values = rows[...].astype(f32)
    scale = lax.rsqrt(jnp.mean(values * values, axis=-1, keepdims=True) + eps)
    width = out.shape[1]
    start = pl.multiple_of(index[0] * width, width)
    own = rows[:, pl.ds(start, width)].astype(f32)
    normed = (own * scale * gain[:, pl.ds(start, width)]).astype(bf16)
    matches = slot_hits(routes[...], experts, capacity)
    picker = functools.reduce(jnp.add, matches).astype(bf16)
    out[...] = dot(picker, normed).astype(bf16)


def combiner_kernel(experts, capacity, routes, weights, high, low):
    matches = slot_hits(routes[...], experts, capacity)
    terms = [m * weights[j : j + 1, :] for j, m in enumerate(matches)]
    total = functools.reduce(jnp.add, terms).T
    rounded = total.astype(bf16)
    high[...] = rounded
    low[...] = (total - rounded.astype(f32)).astype(bf16)


def combine_kernel(high, low, results, out):
    out[...] = (dot(high[...], results[...]) + dot(low[...], results[...])).astype(bf16)


def experts_kernel(
    index, x_0, x_1, x_3, x_2a, x_2b, gate_0, up_0, gate_1, up_1, down_0, down_1, me, out, top, bottom, tall, *rest
):
    *outs, sem = rest
    load = pltpu.make_async_copy(down_1.at[0], tall, sem)
    load.start()
    depth = x_0.shape[1]
    parts = gate_0.shape[1] // depth
    rows = (x_0[...], x_1[...], jnp.concatenate([x_2a[...], x_2b[...]], axis=0), x_3[...])
    places = [lax.rem(index[0] + k, parts) * depth for k in range(parts)]

    def projected(weight):
        spans = [pl.ds(pl.multiple_of(p, depth), depth) for p in places]
        return functools.reduce(jnp.add, [dot(r, weight[0, s, :]) for r, s in zip(rows, spans)])

    hidden = [
        (jax.nn.silu(projected(g)) * projected(u)).astype(bf16)
        for g, u in ((gate_0, up_0), (gate_1, up_1))
    ]
    load.wait()
    half, width = top.shape
    n = tall.shape[1] // width
    span = block_of(me, n // 2, n, width)
    piece = dot(hidden[0], down_0[0, :, span]) + dot(hidden[1], tall[:, span])
    top[...] = piece[:half].astype(bf16)
    bottom[...] = piece[half:].astype(bf16)
    for by, block in zip(offsets(n // 2 - 2), outs):
        span = block_of(me, by, n, width)
        piece = dot(hidden[0], down_0[0, :, span]) + dot(hidden[1], tall[:, span])
        block[...] = piece.astype(bf16)
    units = hidden[0].shape[1]
    out[:, :units] = hidden[0]
    out[:, units:] = hidden[1]


def block_of(me, by, n, width):
    return pl.ds(pl.multiple_of(lax.rem(me[0] + by + n, n) * width, width), width)


def offsets(reach):
    return [0] + [sign * k for k in range(1, reach + 1) for sign in (1, -1)]


def far_kernel(far, me, hidden, down_0, down_1, top, bottom, ahead, behind):
    half, width = top.shape
    n, units = down_1.shape[1] // width, down_1.shape[0]

    def piece(by):
        span = block_of(me, by, n, width)
        return dot(hidden[:, :units], down_0[0, :, span]) + dot(hidden[:, units:], down_1[:, span])

    front, back = piece(far), piece(-far)
    ahead[:half] = (front[:half] + top[...].astype(f32)).astype(bf16)
    ahead[half:] = front[half:].astype(bf16)
    behind[:half] = back[:half].astype(bf16)
    behind[half:] = (back[half:] + bottom[...].astype(f32)).astype(bf16)


def sum_kernel(*refs):
    *pieces, out = refs
    out[...] = functools.reduce(jnp.add, [p[...].astype(f32) for p in pieces]).astype(bf16)


def mixer_kernel(index, *refs):
    *pieces, gain, weight, out = refs
    n, width = len(pieces), pieces[0].shape[1]
    values = jnp.concatenate([p[...] for p in pieces], axis=1).astype(f32)
    spans = [
        pl.ds(pl.multiple_of(lax.rem(index[0] + n - k, n) * width, width), width) for k in range(n)
    ]
    gains = jnp.concatenate([gain[:, span] for span in spans], axis=1)
    weights = jnp.concatenate([weight[span, :] for span in spans], axis=0)
    centered = values - jnp.mean(values, axis=-1, keepdims=True)
    scale = lax.rsqrt(jnp.mean(centered * centered, axis=-1, keepdims=True) + eps)
    activated = jax.nn.silu(centered * scale * gains).astype(bf16)
    out[...] = dot(activated, weights).astype(bf16)


def moved(value, by):
    n = lax.axis_size("tp")
    return lax.ppermute(value, "tp", [(i, (i + by) % n) for i in range(n)])


def partner(value):
    return lax.ppermute(value, "core", [(0, 1), (1, 0)])


def params(mib):
    return pltpu.CompilerParams(vmem_limit_bytes=mib << 20)


def cost(flops, moved):
    return pl.CostEstimate(flops=flops, bytes_accessed=moved, transcendentals=0)


def step_on_device(
    value_in,
    gate_in,
    conv_taps,
    chan_gain,
    out_weight,
    second_rows,
    expert_gain,
    routes,
    route_weights,
    gate_w,
    up_w,
    down_w,
):
    n_z, n_core, n_tp = lax.axis_size("z"), lax.axis_size("core"), lax.axis_size("tp")
    experts = n_z
    tokens, width = second_rows.shape
    top = routes.shape[1]
    capacity = 2 * max(1, min(tokens // 2, 3 * tokens * top // (4 * experts)))
    columns = width // n_tp
    slots = experts * capacity
    vmem = pl.BlockSpec(memory_space=pltpu.VMEM)
    smem = pl.BlockSpec(memory_space=pltpu.SMEM)

    routes_t = routes.T
    me = lax.axis_index("tp")
    parts = n_tp // 2
    wide = width // parts
    quarter = lax.rem(me, parts).astype(jnp.int32).reshape(1)
    outgoing = pl.pallas_call(
        functools.partial(dispatch_kernel, experts, capacity),
        grid=(1,),
        out_shape=jax.ShapeDtypeStruct((slots, wide), bf16),
        in_specs=[smem] + [pl.BlockSpec(s, lambda i: (0, 0)) for s in ((top, tokens), (tokens, width), (1, width))],
        out_specs=pl.BlockSpec((slots, wide), lambda i: (0, 0)),
        compiler_params=params(60),
        cost_estimate=cost(10**8, 10**6),
    )(quarter, routes_t, second_rows, expert_gain.reshape(1, -1))
    arrived = lax.all_to_all(
        outgoing.reshape(experts, capacity, wide), "z", split_axis=0, concat_axis=0, tiled=True
    )

    taps = conv_taps.shape[0]
    halo = -(-(taps - 1) // 16) * 16
    glu = (value_in.astype(f32) * jax.nn.sigmoid(gate_in.astype(f32))).astype(bf16)
    length, channels = glu.shape
    n_ep = n_z * n_core
    before = lax.ppermute(
        glu[length - halo :], ("z", "core"), [(i, i + 1) for i in range(n_ep - 1)]
    )
    padded = jnp.concatenate([before, glu], axis=0).astype(f32)
    total = jnp.zeros(glu.shape, f32)
    for offset in range(taps):
        start = halo - taps + 1 + offset
        total = total + conv_taps[offset][None, :] * padded[start : start + length]
    convolved = total.astype(bf16)
    from_back, from_front = {}, {}
    for k in range(parts, 0, -1):
        from_back[k] = moved(convolved, k)
        if 1 < k < parts:
            from_front[k] = moved(convolved, -k)
    from_front[1] = moved(convolved, -1)

    rows = n_z * capacity
    arrived, _ = lax.optimization_barrier((arrived, convolved))
    x_0 = arrived.reshape(rows, wide)
    x_2a, x_2b = moved(x_0[: rows // 2], -2), moved(x_0[rows // 2 :], 2)
    x_1, x_3 = moved(x_0, -1), moved(x_0, 1)
    down_b = partner(down_w)
    gate_b, up_b = partner(gate_w), partner(up_w)
    units = gate_w.shape[2]
    me_ref = me.astype(jnp.int32).reshape(1)
    shape = lambda *dims: jax.ShapeDtypeStruct(dims, bf16)
    far = parts - 1
    near = [shape(rows, columns)] * (2 * far - 1)
    hidden, top, bottom, down_b, own, *sent = pl.pallas_call(
        experts_kernel,
        out_shape=[
            shape(rows, 2 * units),
            shape(rows // 2, columns),
            shape(rows // 2, columns),
            shape(units, width),
        ]
        + near,
        in_specs=[smem] + [vmem] * 10 + [pl.BlockSpec(memory_space=pl.ANY), smem],
        out_specs=[vmem] * (4 + len(near)),
        scratch_shapes=[pltpu.SemaphoreType.DMA],
        compiler_params=params(24),
        cost_estimate=cost(2 * 10**9, 10**7),
    )(quarter, x_0, x_1, x_3, x_2a, x_2b, gate_w, up_w, gate_b, up_b, down_w, down_b, me_ref)
    top, bottom = moved(top, 1), moved(bottom, -1)
    sent += pl.pallas_call(
        functools.partial(far_kernel, far),
        out_shape=[shape(rows, columns)] * 2,
        in_specs=[smem] + [vmem] * 5,
        out_specs=[vmem] * 2,
        compiler_params=params(16),
        cost_estimate=cost(10**9, 10**6),
    )(me_ref, hidden, down_w, down_b, top, bottom)
    pieces = [own]
    for k in range(far, 0, -1):
        pieces += [moved(sent[2 * k - 2], k), moved(sent[2 * k - 1], -k)]
    sums = pl.pallas_call(
        sum_kernel,
        out_shape=shape(rows, columns),
        in_specs=[vmem] * len(pieces),
        out_specs=vmem,
        compiler_params=params(16),
        cost_estimate=cost(10**8, 2 * 10**6),
    )(*pieces)
    results = lax.all_to_all(
        sums.reshape(n_z, capacity, columns), "z", split_axis=0, concat_axis=0, tiled=True
    ).reshape(slots, columns)

    high, low = pl.pallas_call(
        functools.partial(combiner_kernel, experts, capacity),
        out_shape=[jax.ShapeDtypeStruct((tokens, slots), bf16)] * 2,
        in_specs=[vmem] * 2,
        out_specs=[vmem] * 2,
        compiler_params=params(16),
        cost_estimate=cost(10**8, 10**6),
    )(routes_t, route_weights.T)
    routed_rows = pl.pallas_call(
        combine_kernel,
        out_shape=jax.ShapeDtypeStruct((tokens, columns), bf16),
        in_specs=[vmem] * 3,
        out_specs=vmem,
        compiler_params=params(16),
        cost_estimate=cost(10**8, 10**6),
    )(high, low, results)
    step = length // 2
    gathered = [convolved] + [from_back[k] for k in range(1, parts + 1)]
    gathered += [from_front[k] for k in range(parts - 1, 0, -1)]
    mixer_rows = pl.pallas_call(
        mixer_kernel,
        grid=(length // step,),
        out_shape=jax.ShapeDtypeStruct((length, out_weight.shape[1]), bf16),
        in_specs=[smem]
        + [pl.BlockSpec((step, channels), lambda i: (i, 0))] * n_tp
        + [
            pl.BlockSpec((1, n_tp * channels), lambda i: (0, 0)),
            pl.BlockSpec(out_weight.shape, lambda i: (0, 0)),
        ],
        out_specs=pl.BlockSpec((step, out_weight.shape[1]), lambda i: (i, 0)),
        compiler_params=params(16),
        cost_estimate=cost(10**9, 2 * 10**6),
    )(me.astype(jnp.int32).reshape(1), *gathered, chan_gain.reshape(1, -1), out_weight)
    return (mixer_rows, routed_rows)


def solution(mesh):
    n_grp, n_ep, n_tp = (mesh.shape[name] for name in ("grp", "ep", "tp"))
    finer = Mesh(mesh.devices.reshape(n_grp, n_ep // 2, 2, n_tp), ("grp", "z", "core", "tp"))
    tok = ("grp", "z", "core")
    placed = (
        P(tok, "tp"),
        P(tok, "tp"),
        P(None, "tp"),
        P(),
        P(None, "tp"),
        P(tok, None),
        P(),
        P(tok, None),
        P(tok, None),
        P(("z", "core"), None, "tp"),
        P(("z", "core"), None, "tp"),
        P(("z", "core"), "tp", None),
    )
    return jax.shard_map(
        step_on_device,
        mesh=finer,
        in_specs=placed,
        out_specs=(P(tok, "tp"), P(tok, "tp")),
        check_vma=False,
    )
```
